32 devices in a mesh: sp: 8 (over z, y), tp: 4 (over x, core).
Axes of the slice: x: 2, y: 2, z: 4, core: 2. Of those that a mesh axis runs over, the one named last changes fastest.
Arguments:
- residual: bfloat16 [2048, 2048], P(('sp', 'tp')), may hold values from -6 to 6
- queries: bfloat16 [2048, 2048], P('sp', 'tp'), may hold values from -40 to 40
- key_rows: bfloat16 [2048, 1024], P('sp', 'tp'), may hold values from -40 to 40
- value_rows: bfloat16 [2048, 1024], P('sp', 'tp'), may hold values from -6 to 6
- forget_sums: float32 [2048, 16], P('sp', 'tp'), as said below
- out_weight: bfloat16 [2048, 2048], P('tp'), may hold values from -0.25 to 0.25
- norm_gain: float32 [2048], replicated, may hold values from 0.1 to 1.9
- expert_ids: int32 [2048, 4], P(('sp', 'tp')), may hold values from 0 to 7, all different within a row; in each aligned block of 64 rows (0 to 63, 64 to 127, ...) at most 64 rows name the same one
- route_weights: float32 [2048, 4], P(('sp', 'tp')), may hold values from 0.1 to 1
- expert_gate: bfloat16 [8, 2048, 384], P('sp'), may hold values from -0.125 to 0.125
- expert_up: bfloat16 [8, 2048, 384], P('sp'), may hold values from -0.125 to 0.125
- expert_down: bfloat16 [8, 384, 2048], P('sp'), may hold values from -0.3125 to 0.3125
- shared_gate: bfloat16 [2048, 384], replicated, may hold values from -0.125 to 0.125
- shared_up: bfloat16 [2048, 384], replicated, may hold values from -0.125 to 0.125
- shared_down: bfloat16 [384, 2048], replicated, may hold values from -0.3125 to 0.3125
Outputs:
- layer_out: bfloat16 [2048, 2048], P(('sp', 'tp'))
The draws below stay inside these ranges and needn't reach their ends.
Inputs may be any that keep to these rules, and one draw needn't show every extreme that they name: `forget_sums`: each head's column never rises from one position to the next. `expert_ids`: each row names 4 different experts; among the rows of one device no expert is named more than 64 times.
All inputs are finite; a program needn't handle non-finite values.
Results may differ from the reference program's by a relative error of at most 0.014.
Values may be sent and summed in bfloat16 or wider, within the bound.
A program may use at most 128 MiB of HBM per device.

```python
import math
import jax
import jax.numpy as jnp
import numpy as np
from jax import lax

D = 2048
HEADS = 16
KV_HEADS = 8
HEAD_DIM = 128
FE = 384
FS = 384
TOPK = 4
TOK_DEV = 256
EXPERTS = 8
TOKENS = 2048
ROWS = 64
CAP = 64


def query_key_pair(key):
    base_seed = jax.random.fold_in(key, 11)
    seed_list = jax.random.split(base_seed, 2)
    query_rows = 1.3 * jax.random.normal(seed_list[0], (TOKENS, HEADS * HEAD_DIM), jnp.float32)
    key_block = 1.3 * jax.random.normal(seed_list[1], (TOKENS, KV_HEADS * HEAD_DIM), jnp.float32)
    return (jnp.clip(query_rows, -40.0, 40.0), jnp.clip(key_block, -40.0, 40.0))


def draw_queries(key, part):
    return query_key_pair(key)[0].astype(jnp.bfloat16)


def draw_key_rows(key, part):
    return query_key_pair(key)[1].astype(jnp.bfloat16)


def draw_forget_sums(key, part):
    base_seed = jax.random.fold_in(key, 23)
    seed_list = jax.random.split(base_seed, 7)
    ordering = jax.random.permutation(seed_list[0], HEADS)
    slowly = ordering < HEADS // 2
    slow_rate = jax.random.uniform(seed_list[1], (HEADS,), jnp.float32, 0.25, 1.0) / TOKENS
    fast_rate = jnp.exp(jax.random.uniform(seed_list[2], (HEADS,), jnp.float32, math.log(0.01), math.log(1.0 / 30.0)))
    rates = jnp.where(slowly, slow_rate, fast_rate)
    block_count = TOKENS // TOK_DEV
    factor = jnp.exp(jax.random.uniform(seed_list[3], (block_count, 1), jnp.float32, -0.7, 0.7))
    factor = jnp.repeat(factor, TOK_DEV, axis=0)
    rough = jax.random.uniform(seed_list[4], (TOKENS, HEADS), jnp.float32, 0.2, 1.8)
    log_steps = -rates[None, :] * factor * rough
    places = jax.random.randint(seed_list[5], (3,), 0, TOKENS)
    losses = jnp.log(jax.random.uniform(seed_list[6], (3, HEADS), jnp.float32, 0.5, 0.8))
    log_steps = log_steps.at[places].add(jnp.where(slowly[None, :], losses, 0.0))
    return jnp.cumsum(log_steps, axis=0)


def block_levels(rng, dims, pieces, smallest, high):
    factor_of, own = 1.0, jax.random.fold_in(rng, 6)
    for dim, parts in pieces:
        heights = jnp.exp(jax.random.uniform(jax.random.fold_in(own, dim), (parts,), jnp.float32, smallest / len(pieces), high / len(pieces)))
        factor_of = factor_of * jnp.repeat(heights, dims[dim] // parts).reshape([-1 if axis == dim else 1 for axis in range(len(dims))])
    return factor_of


def assign_block(own_key, own, number, rows, count, top, most, skew):
    sequence = jax.random.permutation(own_key, count)
    crowded, common = load_shares(count, rows * top, most, skew, True), load_shares(count, rows * top, most, skew, False)
    places = jnp.arange(count)

    def named(lengths, rotation):
        used = int((lengths > 0).sum())
        fixed = max(1, used // 4)
        moved = fixed + (places - fixed + rotation * (used - fixed)) % max(1, count - fixed)
        return jnp.zeros((count,), jnp.int32).at[sequence[jnp.where(places < fixed, places, moved)]].set(jnp.asarray(lengths, jnp.int32))

    lengths = jnp.where(number % 4 == 0, named(crowded, number // 4), named(common, number - number // 4 - 1))
    mixed = jax.random.permutation(jax.random.fold_in(own, 3), count)
    source_of, receiver = mixed[0:count // 2 * 2:2], mixed[1:count // 2 * 2:2]
    margin = jnp.minimum(lengths[source_of] - 1, most - lengths[receiver]) // 2
    margin = jnp.where((source_of == sequence[0]) | (receiver == sequence[0]) | (lengths[receiver] == 0), 0, jnp.maximum(margin, 0))
    moved = jax.random.randint(jax.random.fold_in(own, 4), (count // 2,), 0, 1 << 20) % (margin + 1)
    lengths = lengths.at[source_of].add(-moved).at[receiver].add(moved)
    labels = jnp.searchsorted(jnp.cumsum(lengths), jnp.arange(rows * top), side="right").astype(jnp.int32)
    grid = labels.reshape(top, rows).T
    grid = grid[jax.random.permutation(jax.random.fold_in(own, 1), rows)]
    rotation = jax.random.randint(jax.random.fold_in(own, 2), (rows, 1), 0, top)
    return jnp.take_along_axis(grid, (jnp.arange(top)[None, :] + rotation) % top, axis=1)


def load_shares(count, total, reach, lean, full):
    weights = [(1 << 20) // math.isqrt(grade ** lean) + 1 for grade in range(1, count + 1)]
    largest = reach if full else min(reach, max(-(-total // count), total * weights[0] // sum(weights)))
    least = 1 if total - largest >= count - 1 else 0
    given, surplus = [largest] + [least] * (count - 1), total - largest - least * (count - 1)
    while surplus > 0:
        free = [i for i in range(1, count) if given[i] < largest] or [i for i in range(1, count) if given[i] < reach]
        whole, budget = sum([weights[i] for i in free]), surplus
        for i in free:
            more = min(reach - given[i], max(1, budget * weights[i] // whole), surplus)
            given[i] = given[i] + more
            surplus = surplus - more
    return np.array(given)


def scatter_about(own_key, extent, scale, limit, cuts=(), held_as=jnp.bfloat16):
    values = scale * jax.random.normal(own_key, extent, jnp.float32)
    if cuts:
        values = values * block_levels(own_key, extent, cuts, -0.22, 0.18)
    return jnp.clip(values, -limit, limit).astype(held_as)


def setup_inputs(seed: int = 0) -> dict:
    splits = jax.random.split(jax.random.key(seed), 16)
    residual = scatter_about(splits[0], (TOKENS, D), 1.0, 6.0, ((0, 32),))
    queries = draw_queries(jax.random.fold_in(splits[15], 71), 0)
    key_rows = draw_key_rows(jax.random.fold_in(splits[15], 71), 0)
    value_rows = scatter_about(splits[3], (TOKENS, KV_HEADS * HEAD_DIM), 1.0, 6.0, ((0, 8), (1, 4)))
    forget_sums = draw_forget_sums(jax.random.fold_in(splits[15], 71), 0)
    out_weight = scatter_about(splits[5], (HEADS * HEAD_DIM, D), (HEADS * HEAD_DIM // 4) ** -0.5, 0.25, ((0, 4),))
    norm_gain = jnp.clip(1.0 + 0.18 * jax.random.normal(splits[6], (D,), jnp.float32), 0.1, 1.9)
    expert_ids_keys = jax.random.split(jax.random.fold_in(splits[7], 1), TOKENS // ROWS)
    expert_ids_turns = jax.random.permutation(jax.random.fold_in(splits[7], 3), TOKENS // ROWS)
    expert_ids = jax.vmap(lambda own, number: assign_block(jax.random.fold_in(splits[7], 2), own, number, ROWS, EXPERTS, TOPK, CAP, 2))(expert_ids_keys, expert_ids_turns).reshape((TOKENS, TOPK))
    route_weights = jnp.clip(jnp.exp(math.log(1.0) - 2.3025851 * jax.random.uniform(splits[8], (TOKENS, TOPK), jnp.float32) ** block_levels(splits[8], (TOKENS, TOPK), ((0, 32),), -0.2, 0.2)), 0.1, 1.0)
    expert_gate = scatter_about(splits[9], (EXPERTS, D, FE), D ** -0.5, 0.125, ((0, 8),))
    expert_up = scatter_about(splits[10], (EXPERTS, D, FE), D ** -0.5, 0.125, ((0, 8),))
    expert_down = scatter_about(splits[11], (EXPERTS, FE, D), FE ** -0.5, 0.3125, ((0, 8),))
    shared_gate = scatter_about(splits[12], (D, FS), D ** -0.5, 0.125)
    shared_up = scatter_about(splits[13], (D, FS), D ** -0.5, 0.125)
    shared_down = scatter_about(splits[14], (FS, D), FS ** -0.5, 0.3125)
    return {"residual": residual, "queries": queries, "key_rows": key_rows, "value_rows": value_rows, "forget_sums": forget_sums, "out_weight": out_weight, "norm_gain": norm_gain, "expert_ids": expert_ids, "route_weights": route_weights, "expert_gate": expert_gate, "expert_up": expert_up, "expert_down": expert_down, "shared_gate": shared_gate, "shared_up": shared_up, "shared_down": shared_down}


routed_scale = 2.5
norm_eps = 1e-06

def attend(queries, key_rows, value_rows, forget_sums):
    group_size = HEADS // KV_HEADS
    score_scale = HEAD_DIM ** (-0.5)
    key_heads = key_rows.astype(jnp.float32).reshape(TOKENS, KV_HEADS, HEAD_DIM)
    value_heads = value_rows.astype(jnp.float32).reshape(TOKENS, KV_HEADS, HEAD_DIM)
    key_sums = forget_sums.reshape(TOKENS, KV_HEADS, group_size).transpose(1, 2, 0)
    positions = jnp.arange(TOKENS, dtype=jnp.int32)
    block_rows = math.gcd(TOKENS, 256)

    def one_block(first_pos):
        query_block = lax.dynamic_slice_in_dim(queries, first_pos, block_rows, 0).astype(jnp.float32)
        query_block = query_block.reshape(block_rows, KV_HEADS, group_size, HEAD_DIM)
        query_sums = lax.dynamic_slice_in_dim(forget_sums, first_pos, block_rows, 0)
        query_sums = query_sums.reshape(block_rows, KV_HEADS, group_size).transpose(1, 2, 0)
        scores = jnp.einsum('qhgd,khd->hgqk', query_block, key_heads) * score_scale
        scores = scores + (query_sums[:, :, :, None] - key_sums[:, :, None, :])
        query_pos = first_pos + jnp.arange(block_rows, dtype=jnp.int32)
        allowed = query_pos[:, None] >= positions[None, :]
        scores = jnp.where(allowed, scores, -jnp.inf)
        row_max = lax.optimization_barrier(jnp.max(scores, axis=3, keepdims=True))
        weights = jnp.exp(scores - row_max)
        weight_sum = lax.optimization_barrier(jnp.sum(weights, axis=3))
        rounded = lax.optimization_barrier(weights.astype(jnp.bfloat16)).astype(jnp.float32)
        mixed = jnp.einsum('hgqk,khd->qhgd', rounded, value_heads)
        mixed = mixed / weight_sum.transpose(2, 0, 1)[:, :, :, None]
        return mixed.reshape(block_rows, HEADS * HEAD_DIM).astype(jnp.bfloat16)
    starts = jnp.arange(TOKENS // block_rows, dtype=jnp.int32) * block_rows
    return lax.map(one_block, starts).reshape(TOKENS, HEADS * HEAD_DIM)

def experts_all(normed, expert_ids, route_weights, expert_gate, expert_up, expert_down):
    slot_count = TOKENS // ROWS * CAP
    flat_ids = expert_ids.reshape(-1)
    assigned = flat_ids.shape[0]
    gates = route_weights / lax.optimization_barrier(jnp.sum(route_weights, axis=1, keepdims=True)) * routed_scale
    flat_gates = jnp.concatenate([gates.reshape(-1), jnp.zeros((1,), jnp.float32)])
    padded = jnp.concatenate([normed, jnp.zeros((1, D), jnp.bfloat16)])

    def one_expert(carried, expert):
        chosen = flat_ids == expert
        place = jnp.where(chosen, jnp.cumsum(chosen.astype(jnp.int32)) - 1, slot_count)
        source = jnp.full((slot_count + 1,), assigned, jnp.int32)
        source = source.at[place].set(jnp.arange(assigned, dtype=jnp.int32))[:slot_count]
        token_rows = padded[source // TOPK]
        gate_part = jnp.dot(token_rows, expert_gate[expert], preferred_element_type=jnp.float32)
        up_part = jnp.dot(token_rows, expert_up[expert], preferred_element_type=jnp.float32)
        hidden = (jax.nn.silu(gate_part) * up_part).astype(jnp.bfloat16)
        output = jnp.dot(hidden, expert_down[expert], preferred_element_type=jnp.float32).astype(jnp.bfloat16)
        carried = carried.at[source // TOPK].add(flat_gates[source][:, None] * output.astype(jnp.float32))
        return (carried, None)
    routed, _ = lax.scan(one_expert, jnp.zeros((TOKENS + 1, D), jnp.float32), jnp.arange(EXPERTS, dtype=jnp.int32))
    return routed[:TOKENS]

def reference(residual, queries, key_rows, value_rows, forget_sums, out_weight, norm_gain, expert_ids, route_weights, expert_gate, expert_up, expert_down, shared_gate, shared_up, shared_down):
    attended = attend(queries, key_rows, value_rows, forget_sums)
    branch = jnp.dot(attended, out_weight, preferred_element_type=jnp.float32)
    stream = (residual.astype(jnp.float32) + branch).astype(jnp.bfloat16)
    wide = lax.optimization_barrier(stream).astype(jnp.float32)
    normed = (wide * lax.rsqrt(lax.optimization_barrier(jnp.mean(wide * wide, axis=1, keepdims=True)) + norm_eps) * norm_gain).astype(jnp.bfloat16)
    routed = experts_all(normed, expert_ids, route_weights, expert_gate, expert_up, expert_down)
    shared_hidden = (jax.nn.silu(jnp.dot(normed, shared_gate, preferred_element_type=jnp.float32)) * jnp.dot(normed, shared_up, preferred_element_type=jnp.float32)).astype(jnp.bfloat16)
    shared_out = jnp.dot(shared_hidden, shared_down, preferred_element_type=jnp.float32)
    return (wide + shared_out + routed).astype(jnp.bfloat16)
```

```python
import functools
import math
import types

import jax
import jax.numpy as jnp
from jax import lax
from jax.experimental import pallas as pl
from jax.experimental.pallas import tpu as pltpu
from jax.sharding import PartitionSpec as P

HEADS = 16
KV_HEADS = 8
HEAD_DIM = 128
TOPK = 4


routed_scale = 2.5
norm_eps = 1e-06


MESH_ID = pl.DeviceIdType.MESH
LOG2E = math.log2(math.e)


def remote(src, dst, send_sem, recv_sem, target):
    return pltpu.make_async_remote_copy(
        src_ref=src,
        dst_ref=dst,
        send_sem=send_sem,
        recv_sem=recv_sem,
        device_id=target,
        device_id_type=MESH_ID,
    )


def greet(barrier, target):
    pl.semaphore_signal(barrier, inc=1, device_id=target, device_id_type=MESH_ID)


PIECES = 8
ROW_PIECES = 4


def aligned(start, size):
    return pl.ds(pl.multiple_of(start, size), size)


def layer_kernel(names, sp_count, score_scale, *refs):
    r = types.SimpleNamespace(**dict(zip(names, refs)))
    me, tp = lax.axis_index("sp"), lax.axis_index("tp")
    line = sp_count // 2
    last = line - 1
    z, y = me // 2, me % 2
    x, c = tp // 2, tp % 2
    mate_block = 2 * z + 1 - y
    mate = (mate_block, tp)
    above = (jnp.minimum(me + 2, sp_count - 1), tp)
    below = (jnp.maximum(me - 2, 0), tp)
    core_mate = (me, 2 * x + 1 - c)
    x_mate = (me, 2 * (1 - x) + c)
    not_last, not_first = z < last, z > 0
    q_rows = r.q_hbm.shape[0]
    rows, width = r.res_ref.shape
    f32, bf16 = jnp.float32, jnp.bfloat16

    barrier = pltpu.get_barrier_semaphore()
    for peer in (mate, core_mate, x_mate):
        greet(barrier, peer)

    @pl.when(not_last)
    def _():
        greet(barrier, above)

    @pl.when(not_first)
    def _():
        greet(barrier, below)

    def lanes(ref, head):
        return ref.at[:, aligned(head * HEAD_DIM, HEAD_DIM)]

    def q_part(ref, j):
        return ref.at[pl.ds(j * q_rows, q_rows), :]

    loads = [
        (lanes(r.k_hbm, 1 - y), r.ksend),
        (lanes(r.v_hbm, 1 - y), r.vsend),
        (lanes(r.k_hbm, y), r.kbuf.at[me]),
        (lanes(r.v_hbm, y), r.vbuf.at[me]),
        (lanes(r.q_hbm, 2 * (1 - y)), q_part(r.qsend, 0)),
        (lanes(r.q_hbm, 2 * (1 - y) + 1), q_part(r.qsend, 1)),
        (lanes(r.q_hbm, 2 * y), q_part(r.qs.at[y], 0)),
        (lanes(r.q_hbm, 2 * y + 1), q_part(r.qs.at[y], 1)),
    ]
    loads = [pltpu.make_async_copy(a, b, r.load_sem.at[i]) for i, (a, b) in enumerate(loads)]
    for copy in loads:
        copy.start()
    sources = (r.wo_hbm, r.eg_hbm, r.eu_hbm, r.ed_hbm, r.sg_hbm, r.su_hbm, r.sd_hbm)
    held = (r.wo, r.eg.at[0], r.eu.at[0], r.ed.at[0], r.sg, r.su, r.sd)
    weights = [pltpu.make_async_copy(a, b, r.weight_sem.at[i]) for i, (a, b) in enumerate(zip(sources, held))]
    first_f, second_f = r.f_ref[0:2, :], r.f_ref[2:4, :]
    r.fsend[...] = jnp.zeros(r.fsend.shape, f32)
    r.fbuf[me] = jnp.zeros(r.fsend.shape, f32)
    r.fsend[0:2, :] = jnp.where(y == 0, second_f, first_f)
    r.fbuf[me, 0:2, :] = jnp.where(y == 0, first_f, second_f)
    scores = r.score_ref[...]
    gates = scores / jnp.sum(scores, axis=0, keepdims=True) * routed_scale
    for e in range(sp_count):
        r.gbuf[z, e : e + 1, :] = jnp.sum(jnp.where(r.ids_ref[...] == e, gates, 0.0), axis=0, keepdims=True)
    r.acc[...] = jnp.zeros(r.acc.shape, f32)
    r.den[...] = jnp.zeros(r.den.shape, f32)
    r.top[...] = jnp.full(r.top.shape, -jnp.inf, f32)
    for copy in loads:
        copy.wait()
    pl.semaphore_wait(barrier, 3 + not_last.astype(jnp.int32) + not_first.astype(jnp.int32))

    def side_moves(block, sources):
        bufs = (r.fbuf, r.kbuf, r.vbuf)
        return [
            remote(a, b.at[block], r.side_send.at[i], r.kv_recv.at[block, i], mate)
            for i, (a, b) in enumerate(zip(sources, bufs))
        ]

    def up_moves(block, target):
        return [
            remote(b.at[block], b.at[block], r.kv_send.at[block, i], r.kv_recv.at[block, i], target)
            for i, b in enumerate((r.fbuf, r.kbuf, r.vbuf))
        ]

    def pass_up(block):
        @pl.when(not_last)
        def _():
            for copy in up_moves(block, above):
                copy.start()

    def q_move(slot):
        return remote(r.qsend, r.qs.at[slot], r.side_send.at[3], r.q_recv.at[0], mate)

    def parts(refs, quarter, i):
        g, u, d = refs
        tall, flat, wide = g.shape[0] // 4 // PIECES, d.shape[0] // 4, d.shape[1] // PIECES
        span = aligned((quarter * PIECES + i) * tall, tall)
        return (g.at[span, :], u.at[span, :], d.at[aligned(quarter * flat, flat), aligned(i * wide, wide)])

    own_expert = (r.eg_hbm, r.eu_hbm, r.ed_hbm)
    mates_expert = (r.eg.at[1], r.eu.at[1], r.ed.at[1])

    def w_moves(sources, quarter, i, send, recv, target):
        return [
            remote(a, b, send.at[i, k], recv.at[i, k], target)
            for k, (a, b) in enumerate(zip(parts(sources, quarter, i), parts(mates_expert, quarter, i)))
        ]

    def w_side(i):
        return w_moves(own_expert, tp, i, r.wy_send, r.wy_recv, mate)

    def w_hop(i, quarter):
        return w_moves(mates_expert, quarter, i, r.wx_send, r.wx_recv, x_mate)

    def w_core(part, i, quarter):
        return w_moves(mates_expert, quarter, i, r.wc_send.at[part], r.wc_recv.at[part], core_mate)

    x_quarter = 2 * (1 - x) + c

    def issue_weights(start, stop):
        def one(i, _):
            for copy in w_side(i):
                copy.start()
            return 0

        lax.fori_loop(start, stop, one, 0)

    def spread_x(i):
        for copy in w_hop(i, x_quarter):
            copy.wait_recv()
        for copy in w_core(1, i, x_quarter):
            copy.start()

    def spread(start, stop):
        def one(i, _):
            for copy in w_side(i):
                copy.wait_recv()
            for copy in w_hop(i, tp):
                copy.start()
            for copy in w_core(0, i, tp):
                copy.start()

            @pl.when(i >= 2)
            def _():
                spread_x(i - 2)

            return 0

        lax.fori_loop(start, stop, one, 0)

    def at_z(*values):
        out = values[-1]
        for level in range(len(values) - 1):
            out = jnp.where(z == level, values[level], out)
        return out

    early = jnp.maximum(2 * z - 1, 0)
    for copy in side_moves(me, (r.fsend, r.ksend, r.vsend)):
        copy.start()
    q_move(y).start()
    pass_up(me)
    issue_weights(0, early)
    for copy in weights:
        copy.start()

    def absorb(i, block, masked):
        q_block = 2 * z + i
        keys, values = r.kbuf[block], r.vbuf[block]
        for j in range(2):
            span = slice(j * q_rows, (j + 1) * q_rows)
            products = lax.dot_general(
                keys, r.qs[i, span, :], (((1,), (1,)), ((), ())), preferred_element_type=f32
            )
            column = jnp.broadcast_to(r.fbuf[block, j : j + 1, :], (HEAD_DIM, q_rows)).T
            column = jnp.concatenate([column] * (q_rows // HEAD_DIM), axis=1)
            drop = r.fbuf[q_block, j : j + 1, :] - column
            part = products * (score_scale * LOG2E) + drop * LOG2E
            if masked:
                at_key = lax.broadcasted_iota(jnp.int32, part.shape, 0)
                at_query = lax.broadcasted_iota(jnp.int32, part.shape, 1)
                part = jnp.where(at_query >= at_key, part, -jnp.inf)
            old = r.top[i, :1, span]
            peak = jnp.maximum(old, jnp.max(part, axis=0, keepdims=True))
            factor = jnp.exp2(old - peak)
            w = jnp.exp2(part - peak)
            r.den[i, :1, span] = r.den[i, :1, span] * factor + jnp.sum(w, axis=0, keepdims=True)
            mixed = lax.dot_general(
                values, w.astype(bf16), (((0,), (0,)), ((), ())), preferred_element_type=f32
            )
            r.acc[i, :, span] = r.acc[i, :, span] * factor + mixed
            r.top[i, :1, span] = peak

    absorb(y, me, True)
    for copy in side_moves(mate_block, (r.fsend, r.ksend, r.vsend)):
        copy.wait_recv()
    pass_up(mate_block)
    q_move(1 - y).wait_recv()
    absorb(1 - y, mate_block, True)
    absorb(1, 2 * z, False)

    def take(turn, _):
        level = z - 1 - turn // 2
        block = 2 * level + jnp.where(turn % 2 == 0, y, 1 - y)
        for copy in up_moves(block, below):
            copy.wait_recv()
        pass_up(block)
        absorb(1 - y, block, False)
        absorb(y, block, False)

        @pl.when(jnp.logical_and(z == last, jnp.logical_and(turn >= 3, turn < 5)))
        def _():
            spread(turn - 3, turn - 2)

        return 0

    lax.fori_loop(0, 2 * z, take, 0)

    def finish(i, target):
        for j in range(2):
            span = slice(j * q_rows, (j + 1) * q_rows)
            done = (r.acc[i, :, span] / r.den[i, :1, span]).T
            target[:, j * HEAD_DIM : (j + 1) * HEAD_DIM] = done.astype(bf16)

    def back_move(slot):
        return remote(r.attsend, r.att.at[slot], r.back_sem.at[0], r.back_sem.at[1], mate)

    finish(1 - y, r.attsend)
    back_move(y).start()
    issue_weights(early, PIECES)
    finish(y, r.att.at[y])
    marks = [at_z(0, 0, 0, 2), at_z(0, 1, 2, 3), at_z(0, 1, 3, 5), at_z(3, 3, 5, 7), at_z(5, 4, 6, 8)]
    marks += [at_z(8, 7, 8, 8), PIECES]
    spread(marks[0], marks[1])

    weights[0].wait()
    far, near = (1 - x) * 2, x * 2
    back_move(1 - y).wait_recv()
    half = r.att.shape[2]

    def core_copy(i):
        return remote(r.core_out.at[i], r.core_in.at[i], r.pair_sem.at[0, i], r.pair_sem.at[1, i], core_mate)

    part_rows = rows // ROW_PIECES

    def piece(ref, p):
        return ref.at[pl.ds(p * part_rows, part_rows), :]

    def hop(p):
        return remote(piece(r.x_out, p), piece(r.x_in, p), r.hop_sem.at[0, p], r.hop_sem.at[1, p], x_mate)

    def project_to(i, _):
        out_x = jnp.where(i == 0, far, near)
        span = aligned(out_x * rows, 2 * rows)
        r.pair[...] = jnp.dot(
            r.att[0, span, :], r.wo[0:half, :], preferred_element_type=f32
        ) + jnp.dot(r.att[1, span, :], r.wo[half : 2 * half, :], preferred_element_type=f32)
        r.core_out[i] = r.pair[aligned((1 - c) * rows, rows), :].astype(bf16)
        core_copy(i).start()
        r.kept[...] = r.pair[aligned(c * rows, rows), :]
        core_copy(i).wait_recv()

        @pl.when(i == 0)
        def _():
            for p in range(ROW_PIECES):
                span = slice(p * part_rows, (p + 1) * part_rows)
                r.x_out[span, :] = (r.kept[span, :] + r.core_in[0, span, :].astype(f32)).astype(bf16)
                hop(p).start()

        return 0

    lax.fori_loop(0, 2, project_to, 0)
    spread(marks[1], marks[2])

    def tok_move(level, p, send, target):
        return remote(
            piece(r.tok.at[level], p), piece(r.tok.at[level], p), send.at[level, p], r.tok_recv.at[level, p], target
        )

    def gate_move(level, send, target):
        return remote(r.gbuf.at[level], r.gbuf.at[level], send.at[level], r.gate_recv.at[level], target)

    @pl.when(not_last)
    def _():
        gate_move(z, r.gate_up, above).start()

    @pl.when(not_first)
    def _():
        gate_move(z, r.gate_dn, below).start()

    for p in range(ROW_PIECES):
        span = slice(p * part_rows, (p + 1) * part_rows)
        branch = r.kept[span, :] + r.core_in[1, span, :].astype(f32) + r.res_ref[span, :].astype(f32)
        hop(p).wait_recv()
        stream = (branch + r.x_in[span, :].astype(f32)).astype(bf16)
        wide = stream.astype(f32)
        scale = lax.rsqrt(jnp.mean(wide * wide, axis=1, keepdims=True) + norm_eps)
        r.tok[z, span, :] = (wide * scale * r.gain_ref[...]).astype(bf16)
        r.base[span, :] = wide

        @pl.when(not_last)
        def _():
            tok_move(z, p, r.tok_up, above).start()

        @pl.when(not_first)
        def _():
            tok_move(z, p, r.tok_dn, below).start()

    spread(marks[2], marks[3])
    for copy in weights[1:]:
        copy.wait()

    def gated(inputs, gate, up, down):
        first = jnp.dot(inputs, gate[...], preferred_element_type=f32)
        second = jnp.dot(inputs, up[...], preferred_element_type=f32)
        hidden = (first / (1.0 + jnp.exp(-first)) * second).astype(bf16)
        return jnp.dot(hidden, down[...], preferred_element_type=f32)

    def expert(level, slot, number):
        table = r.gbuf[level]
        at_expert = lax.broadcasted_iota(jnp.int32, table.shape, 0) == number
        row = jnp.sum(jnp.where(at_expert, table, 0.0), axis=0, keepdims=True)
        shape = (rows, row.shape[1])
        diagonal = lax.broadcasted_iota(jnp.int32, shape, 0) == lax.broadcasted_iota(jnp.int32, shape, 1)
        column = jnp.sum(jnp.where(diagonal, row, 0.0), axis=1, keepdims=True)
        result = gated(r.tok[level], r.eg.at[slot], r.eu.at[slot], r.ed.at[slot])
        return result.astype(bf16).astype(f32) * column

    def level_at(k):
        plain = k + (k >= z).astype(jnp.int32)
        swapped = jnp.where(k == last - 1, last - 2, jnp.where(k == last - 2, last, k))
        return jnp.where(z == last - 1, swapped, plain)

    def arrive(level):
        @pl.when(level < z)
        def _():
            gate_move(level, r.gate_up, below).wait_recv()

            @pl.when(not_last)
            def _():
                gate_move(level, r.gate_up, above).start()

            for p in range(ROW_PIECES):
                tok_move(level, p, r.tok_up, below).wait_recv()

                @pl.when(not_last)
                def _():
                    tok_move(level, p, r.tok_up, above).start()

        @pl.when(level > z)
        def _():
            gate_move(level, r.gate_dn, above).wait_recv()

            @pl.when(not_first)
            def _():
                gate_move(level, r.gate_dn, below).start()

            for p in range(ROW_PIECES):
                tok_move(level, p, r.tok_dn, above).wait_recv()

                @pl.when(not_first)
                def _():
                    tok_move(level, p, r.tok_dn, below).start()

    def up_back(level, p):
        return remote(
            piece(r.ret_out.at[level], p), piece(r.up_in.at[level], p), r.ret_send.at[level, p], r.up_recv.at[level, p], above
        )

    def dn_back(level, p):
        return remote(
            piece(r.ret_out.at[level], p), piece(r.dn_in.at[level], p), r.ret_send.at[level, p], r.dn_recv.at[level, p], below
        )

    def give_back(level):
        def send(back, came, chained):
            for p in range(ROW_PIECES):
                span = pl.ds(p * part_rows, part_rows)

                @pl.when(chained)
                def _():
                    back(level, p).wait_recv()
                    r.ret_out[level, span, :] = (
                        r.own[level, span, :] + came[level, span, :].astype(f32)
                    ).astype(bf16)

                @pl.when(jnp.logical_not(chained))
                def _():
                    r.ret_out[level, span, :] = r.own[level, span, :].astype(bf16)

                back(level, p).start()

        @pl.when(level > z)
        def _():
            send(up_back, r.up_in, not_first)

        @pl.when(level < z)
        def _():
            send(dn_back, r.dn_in, not_last)

    at_end = jnp.logical_or(z == 0, z == last)

    def first_turns(k, _):
        level = level_at(k)
        arrive(level)
        spread(jnp.where(k == 0, marks[3], marks[4]), jnp.where(k == 0, marks[4], marks[5]))
        r.own[level] = expert(level, 0, me)
        return 0

    lax.fori_loop(0, line - 2, first_turns, 0)
    spread(marks[5], PIECES)
    r.base[...] += gated(r.tok[z], r.sg, r.su, r.sd)
    spread_x(PIECES - 2)
    spread_x(PIECES - 1)

    def take_core(i, _):
        for copy in w_core(0, i, 2 * x + 1 - c) + w_core(1, i, 2 * (1 - x) + 1 - c):
            copy.wait_recv()
        return 0

    lax.fori_loop(0, PIECES, take_core, 0)

    @pl.when(z == last - 1)
    def _():
        arrive(level_at(line - 2))

    def second_turns(k, _):
        level = jnp.where(k < line - 1, level_at(k), z)

        @pl.when(k >= line - 2)
        def _():
            @pl.when(jnp.logical_and(k == line - 2, z != last - 1))
            def _():
                arrive(level)

            r.own[level] = expert(level, 0, me)

        r.own[level] += expert(level, 1, mate_block)

        @pl.when(jnp.logical_and(k < line - 1, at_end))
        def _():
            give_back(level)

        return 0

    lax.fori_loop(0, line, second_turns, 0)
    r.base[...] += r.own[z]

    def middle(k, _):
        @pl.when(jnp.logical_not(at_end))
        def _():
            order = jnp.where(
                z == last - 1,
                jnp.where(k < line - 2, k, last),
                jnp.where(k == 0, last - 1, jnp.where(k == 1, 0, last)),
            )
            give_back(order)

        return 0

    lax.fori_loop(0, line - 1, middle, 0)

    @pl.when(not_first)
    def _():
        for p in range(ROW_PIECES):
            up_back(z, p).wait_recv()
        r.base[...] += r.up_in[z].astype(f32)

    @pl.when(not_last)
    def _():
        for p in range(ROW_PIECES):
            dn_back(z, p).wait_recv()
        r.base[...] += r.dn_in[z].astype(f32)

    r.out_ref[...] = r.base[...].astype(bf16)

    for copy in side_moves(me, (r.fsend, r.ksend, r.vsend)) + [q_move(y), back_move(y)]:
        copy.wait_send()
    for i in range(2):
        core_copy(i).wait_send()
    for p in range(ROW_PIECES):
        hop(p).wait_send()

    def drain_weights(i, _):
        for copy in w_side(i) + w_hop(i, tp) + w_core(0, i, tp) + w_core(1, i, x_quarter):
            copy.wait_send()
        return 0

    lax.fori_loop(0, PIECES, drain_weights, 0)

    def drain(level, _):
        @pl.when(jnp.logical_and(level <= z, not_last))
        def _():
            for half_block in range(2):
                for copy in up_moves(2 * level + half_block, above):
                    copy.wait_send()
            gate_move(level, r.gate_up, above).wait_send()
            for p in range(ROW_PIECES):
                tok_move(level, p, r.tok_up, above).wait_send()

        @pl.when(jnp.logical_and(level >= z, not_first))
        def _():
            gate_move(level, r.gate_dn, below).wait_send()
            for p in range(ROW_PIECES):
                tok_move(level, p, r.tok_dn, below).wait_send()

        @pl.when(level > z)
        def _():
            for p in range(ROW_PIECES):
                up_back(level, p).wait_send()

        @pl.when(level < z)
        def _():
            for p in range(ROW_PIECES):
                dn_back(level, p).wait_send()

        return 0

    lax.fori_loop(0, line, drain, 0)


def layer_fused(
    residual,
    queries,
    key_rows,
    value_rows,
    forget_sums,
    norm_gain,
    expert_ids,
    route_weights,
    out_weight,
    expert_gate,
    expert_up,
    expert_down,
    shared_gate,
    shared_up,
    shared_down,
    sp_count,
):
    q_rows, features = queries.shape
    rows, width = residual.shape
    line = sp_count // 2
    bf16, f32 = jnp.bfloat16, jnp.float32
    vmem, hbm = pl.BlockSpec(memory_space=pltpu.VMEM), pl.BlockSpec(memory_space=pl.ANY)
    loaded = (
        out_weight,
        expert_gate[0],
        expert_up[0],
        expert_down[0],
        shared_gate,
        shared_up,
        shared_down,
    )
    ins = ["q_hbm", "f_ref", "k_hbm", "v_hbm", "res_ref", "gain_ref", "ids_ref", "score_ref"]
    ins += ["wo_hbm", "eg_hbm", "eu_hbm", "ed_hbm", "sg_hbm", "su_hbm", "sd_hbm"]
    one, per_level = (rows, width), (line, rows, width)
    stacked = (2 * q_rows, HEAD_DIM)

    def buf(*shape):
        return pltpu.VMEM(shape, bf16)

    def wide(*shape):
        return pltpu.VMEM(shape, f32)

    def dma(*shape):
        return pltpu.SemaphoreType.DMA(shape)

    scratch = {
        "qs": buf(2, *stacked),
        "qsend": buf(*stacked),
        "kbuf": buf(sp_count, q_rows, HEAD_DIM),
        "vbuf": buf(sp_count, q_rows, HEAD_DIM),
        "fbuf": wide(sp_count, 8, q_rows),
        "ksend": buf(q_rows, HEAD_DIM),
        "vsend": buf(q_rows, HEAD_DIM),
        "fsend": wide(8, q_rows),
        "acc": wide(2, HEAD_DIM, 2 * q_rows),
        "top": wide(2, 8, 2 * q_rows),
        "den": wide(2, 8, 2 * q_rows),
        "att": buf(2, q_rows, features // 2),
        "attsend": buf(q_rows, features // 2),
        "wo": buf(*out_weight.shape),
        "eg": buf(2, *expert_gate.shape[1:]),
        "eu": buf(2, *expert_up.shape[1:]),
        "ed": buf(2, *expert_down.shape[1:]),
        "sg": buf(*shared_gate.shape),
        "su": buf(*shared_up.shape),
        "sd": buf(*shared_down.shape),
        "gbuf": wide(line, sp_count, rows),
        "pair": wide(2 * rows, width),
        "kept": wide(*one),
        "core_out": buf(2, *one),
        "core_in": buf(2, *one),
        "x_out": buf(*one),
        "x_in": buf(*one),
        "base": wide(*one),
        "tok": buf(*per_level),
        "own": wide(*per_level),
        "ret_out": buf(*per_level),
        "up_in": buf(*per_level),
        "dn_in": buf(*per_level),
        "load_sem": dma(8),
        "weight_sem": dma(7),
        "side_send": dma(4),
        "q_recv": dma(1),
        "kv_send": dma(sp_count, 3),
        "kv_recv": dma(sp_count, 3),
        "back_sem": dma(2),
        "wy_send": dma(PIECES, 3),
        "wy_recv": dma(PIECES, 3),
        "wx_send": dma(PIECES, 3),
        "wx_recv": dma(PIECES, 3),
        "wc_send": dma(2, PIECES, 3),
        "wc_recv": dma(2, PIECES, 3),
        "pair_sem": dma(2, 2),
        "hop_sem": dma(2, ROW_PIECES),
        "tok_up": dma(line, ROW_PIECES),
        "tok_dn": dma(line, ROW_PIECES),
        "tok_recv": dma(line, ROW_PIECES),
        "gate_up": dma(line),
        "gate_dn": dma(line),
        "gate_recv": dma(line),
        "ret_send": dma(line, ROW_PIECES),
        "up_recv": dma(line, ROW_PIECES),
        "dn_recv": dma(line, ROW_PIECES),
    }
    names = ins + ["out_ref"] + list(scratch)
    return pl.pallas_call(
        functools.partial(layer_kernel, names, sp_count, HEAD_DIM ** (-0.5)),
        out_shape=jax.ShapeDtypeStruct(one, bf16),
        in_specs=[hbm, vmem, hbm, hbm] + [vmem] * 4 + [hbm] * 7,
        out_specs=vmem,
        scratch_shapes=list(scratch.values()),
        compiler_params=pltpu.CompilerParams(
            collective_id=0, has_side_effects=True, vmem_limit_bytes=60 * 2**20
        ),
    )(
        queries,
        forget_sums.T,
        key_rows,
        value_rows,
        residual,
        norm_gain[None, :],
        expert_ids.T,
        route_weights.T,
        *loaded,
    )


def absorb_group(carried, query_group, shard_piece, sum_piece, score_scale):
    query_heads, query_sums, query_pos, last_pos = query_group
    key_piece, value_piece = shard_piece
    piece_rows = key_piece.shape[0]
    query_count, local_kv, group_size, head_size = query_heads.shape
    key_block = math.gcd(piece_rows, 1024)
    key_heads = key_piece.reshape(piece_rows, local_kv, head_size)
    value_heads = value_piece.reshape(piece_rows, local_kv, head_size)
    key_sums = sum_piece.reshape(piece_rows, local_kv, group_size).transpose(1, 2, 0)

    def update(block_start, held):
        row_max, row_sum, weighted = held
        key_part = lax.dynamic_slice_in_dim(key_heads, block_start, key_block, 0)
        value_part = lax.dynamic_slice_in_dim(value_heads, block_start, key_block, 0)
        sums_part = lax.dynamic_slice_in_dim(key_sums, block_start, key_block, 2)
        scores = (
            jnp.einsum("qhgd,khd->hgqk", query_heads, key_part, preferred_element_type=jnp.float32)
            * score_scale
        )
        scores = scores + (query_sums[:, :, :, None] - sums_part[:, :, None, :])
        key_pos = block_start + jnp.arange(key_block, dtype=jnp.int32)
        allowed = query_pos[:, None] >= key_pos[None, :]
        scores = jnp.where(allowed, scores, -jnp.inf)
        new_max = jnp.maximum(row_max, jnp.max(scores, axis=3))
        weights = jnp.exp(scores - new_max[:, :, :, None])
        factor = jnp.exp(row_max - new_max)
        row_sum = row_sum * factor + jnp.sum(weights, axis=3)
        products = jnp.einsum(
            "hgqk,khd->qhgd",
            weights.astype(jnp.bfloat16),
            value_part,
            preferred_element_type=jnp.float32,
        )
        weighted = weighted * factor.transpose(2, 0, 1)[:, :, :, None] + products
        return (new_max, row_sum, weighted)

    def one_block(block_index, held):
        block_start = block_index * key_block
        needed = block_start <= last_pos
        return lax.cond(needed, lambda inner: update(block_start, inner), lambda inner: inner, held)

    return lax.fori_loop(0, piece_rows // key_block, one_block, carried)


def finish(carried):
    row_max, row_sum, weighted = carried
    mixed = weighted / row_sum.transpose(2, 0, 1)[:, :, :, None]
    return mixed.reshape(mixed.shape[0], -1).astype(jnp.bfloat16)


def local(
    residual,
    queries,
    key_rows,
    value_rows,
    forget_sums,
    out_weight,
    norm_gain,
    expert_ids,
    route_weights,
    expert_gate,
    expert_up,
    expert_down,
    shared_gate,
    shared_up,
    shared_down,
):
    sp_count = lax.axis_size("sp")
    sp_index = lax.axis_index("sp")
    local_rows = queries.shape[0]
    local_kv = key_rows.shape[1] // HEAD_DIM
    group_size = HEADS // KV_HEADS
    score_scale = HEAD_DIM ** (-0.5)
    tp_count = lax.axis_size("tp")
    tokens_here = residual.shape[0]
    every_slot = 2 * tokens_here * TOPK >= tokens_here * expert_gate.shape[0] * sp_count
    if every_slot and expert_gate.shape[0] == 1 and sp_count == 8 and tp_count == 4:
        return layer_fused(
            residual,
            queries,
            key_rows,
            value_rows,
            forget_sums,
            norm_gain,
            expert_ids,
            route_weights,
            out_weight,
            expert_gate,
            expert_up,
            expert_down,
            shared_gate,
            shared_up,
            shared_down,
            sp_count,
        )
    own_first = sp_index * local_rows
    all_sums = lax.all_gather(forget_sums, "sp", axis=0, tiled=True)
    positions = own_first + jnp.arange(local_rows, dtype=jnp.int32)
    groups = [
        (
            queries.reshape(queries.shape[0], local_kv, group_size, HEAD_DIM),
            forget_sums.reshape(forget_sums.shape[0], local_kv, group_size).transpose(1, 2, 0),
            positions,
            positions[-1],
        )
    ]

    def initial(query_count):
        return (
            jnp.full((local_kv, group_size, query_count), -1e30, jnp.float32),
            jnp.zeros((local_kv, group_size, query_count), jnp.float32),
            jnp.zeros((query_count, local_kv, group_size, HEAD_DIM), jnp.float32),
        )

    def absorb(states, shard_piece):
        return tuple(
            (
                absorb_group(held, query_group, shard_piece, all_sums, score_scale)
                for held, query_group in zip(states, groups)
            )
        )

    start_states = tuple((initial(query_group[0].shape[0]) for query_group in groups))
    states = absorb(
        start_states,
        (
            lax.all_gather(key_rows, "sp", axis=0, tiled=True),
            lax.all_gather(value_rows, "sp", axis=0, tiled=True),
        ),
    )
    outputs = [finish(held) for held in states]
    attended = outputs[0]
    rows_out = local_rows // lax.axis_size("tp")
    branch = lax.psum_scatter(
        jnp.dot(attended, out_weight, preferred_element_type=jnp.float32).astype(jnp.bfloat16),
        "tp",
        scatter_dimension=0,
        tiled=True,
    ).astype(jnp.float32)
    stream = (residual.astype(jnp.float32) + branch).astype(jnp.bfloat16)
    wide = lax.optimization_barrier(stream).astype(jnp.float32)
    normed = (
        wide * lax.rsqrt(jnp.mean(wide * wide, axis=1, keepdims=True) + norm_eps) * norm_gain
    ).astype(jnp.bfloat16)
    width = normed.shape[1]
    experts_here = expert_gate.shape[0]
    total_experts = experts_here * sp_count
    capacity = 2 * rows_out * TOPK // total_experts
    flat_ids = expert_ids.reshape(-1)
    assigned = flat_ids.shape[0]
    onehot = (flat_ids[:, None] == jnp.arange(total_experts, dtype=jnp.int32)[None, :]).astype(
        jnp.int32
    )
    slot_rank = jnp.sum((jnp.cumsum(onehot, axis=0) - 1) * onehot, axis=1)
    target = flat_ids * capacity + slot_rank
    slot_count = total_experts * capacity
    source = (
        jnp.full((slot_count,), assigned, jnp.int32)
        .at[target]
        .set(jnp.arange(assigned, dtype=jnp.int32))
    )
    padded = jnp.concatenate([normed, jnp.zeros((1, width), jnp.bfloat16)], axis=0)
    outgoing = padded[source // TOPK].reshape(sp_count, experts_here, capacity, width)
    arrived = lax.all_to_all(outgoing, "sp", split_axis=0, concat_axis=0, tiled=True)
    gate_part = jnp.einsum(
        "necd,edf->necf", arrived, expert_gate, preferred_element_type=jnp.float32
    )
    up_part = jnp.einsum("necd,edf->necf", arrived, expert_up, preferred_element_type=jnp.float32)
    hidden = (jax.nn.silu(gate_part) * up_part).astype(jnp.bfloat16)
    processed = jnp.einsum(
        "necf,efd->necd", hidden, expert_down, preferred_element_type=jnp.float32
    ).astype(jnp.bfloat16)
    returned = lax.all_to_all(processed, "sp", split_axis=0, concat_axis=0, tiled=True)
    results = returned.reshape(slot_count, width)
    picked = results[target].reshape(rows_out, TOPK, width).astype(jnp.float32)
    gates = route_weights / jnp.sum(route_weights, axis=1, keepdims=True) * routed_scale
    routed = jnp.sum(gates[:, :, None] * picked, axis=1)
    shared_hidden = (
        jax.nn.silu(jnp.dot(normed, shared_gate, preferred_element_type=jnp.float32))
        * jnp.dot(normed, shared_up, preferred_element_type=jnp.float32)
    ).astype(jnp.bfloat16)
    shared_out = jnp.dot(shared_hidden, shared_down, preferred_element_type=jnp.float32)
    return (wide + shared_out + routed).astype(jnp.bfloat16)


def solution(mesh):
    in_specs = (
        P(("sp", "tp"), None),
        P("sp", "tp"),
        P("sp", "tp"),
        P("sp", "tp"),
        P("sp", "tp"),
        P("tp", None),
        P(),
        P(("sp", "tp"), None),
        P(("sp", "tp"), None),
        P("sp", None, None),
        P("sp", None, None),
        P("sp", None, None),
        P(),
        P(),
        P(),
    )
    out_specs = P(("sp", "tp"), None)
    return jax.shard_map(local, mesh=mesh, in_specs=in_specs, out_specs=out_specs, check_vma=False)
```

```python
import functools
import math
import types

import jax
import jax.numpy as jnp
from jax import lax
from jax.experimental import pallas as pl
from jax.experimental.pallas import tpu as pltpu
from jax.sharding import PartitionSpec as P

HEADS = 16
KV_HEADS = 8
HEAD_DIM = 128
TOPK = 4


routed_scale = 2.5
norm_eps = 1e-06


MESH_ID = pl.DeviceIdType.MESH
LOG2E = math.log2(math.e)


def remote(src, dst, send_sem, recv_sem, target):
    return pltpu.make_async_remote_copy(
        src_ref=src,
        dst_ref=dst,
        send_sem=send_sem,
        recv_sem=recv_sem,
        device_id=target,
        device_id_type=MESH_ID,
    )


def greet(barrier, target):
    pl.semaphore_signal(barrier, inc=1, device_id=target, device_id_type=MESH_ID)


PIECES = 8
EXTRA = 1
ROW_PIECES = 4


def aligned(start, size):
    return pl.ds(pl.multiple_of(start, size), size)


def layer_kernel(names, sp_count, score_scale, *refs):
    r = types.SimpleNamespace(**dict(zip(names, refs)))
    me, tp = lax.axis_index("sp"), lax.axis_index("tp")
    line = sp_count // 2
    last = line - 1
    z, y = me // 2, me % 2
    x, c = tp // 2, tp % 2
    mate_block = 2 * z + 1 - y
    mate = (mate_block, tp)
    above = (jnp.minimum(me + 2, sp_count - 1), tp)
    below = (jnp.maximum(me - 2, 0), tp)
    core_mate = (me, 2 * x + 1 - c)
    x_mate = (me, 2 * (1 - x) + c)
    not_last, not_first = z < last, z > 0
    q_rows = r.q_hbm.shape[0]
    rows, width = r.res_hbm.shape
    f32, bf16 = jnp.float32, jnp.bfloat16

    barrier = pltpu.get_barrier_semaphore()
    for peer in (mate, core_mate, x_mate):
        greet(barrier, peer)

    @pl.when(not_last)
    def _():
        greet(barrier, above)

    @pl.when(not_first)
    def _():
        greet(barrier, below)

    def lanes(ref, head):
        return ref.at[:, aligned(head * HEAD_DIM, HEAD_DIM)]

    def q_part(ref, j):
        return ref.at[pl.ds(j * q_rows, q_rows), :]

    loads = [
        (lanes(r.k_hbm, 1 - y), r.ksend),
        (lanes(r.v_hbm, 1 - y), r.vsend),
        (lanes(r.k_hbm, y), r.kbuf.at[me]),
        (lanes(r.v_hbm, y), r.vbuf.at[me]),
        (lanes(r.q_hbm, 2 * (1 - y)), q_part(r.qsend, 0)),
        (lanes(r.q_hbm, 2 * (1 - y) + 1), q_part(r.qsend, 1)),
        (lanes(r.q_hbm, 2 * y), q_part(r.qs.at[y], 0)),
        (lanes(r.q_hbm, 2 * y + 1), q_part(r.qs.at[y], 1)),
        (r.f_hbm, r.f_ref),
        (r.ids_hbm, r.ids_ref),
        (r.score_hbm, r.score_ref),
        (r.res_hbm, r.res_ref),
        (r.gain_hbm, r.gain_ref),
    ]
    loads = [pltpu.make_async_copy(a, b, r.load_sem.at[i]) for i, (a, b) in enumerate(loads)]
    for copy in loads:
        copy.start()
    sources = (r.wo_hbm, r.eg_hbm, r.eu_hbm, r.ed_hbm, r.sg_hbm, r.su_hbm, r.sd_hbm)
    held = (r.wo, r.eg.at[0], r.eu.at[0], r.ed.at[0], r.sg, r.su, r.sd)
    weights = [pltpu.make_async_copy(a, b, r.weight_sem.at[i]) for i, (a, b) in enumerate(zip(sources, held))]
    r.acc[...] = jnp.zeros(r.acc.shape, f32)
    r.den[...] = jnp.zeros(r.den.shape, f32)
    r.top[...] = jnp.full(r.top.shape, -jnp.inf, f32)
    r.fsend[...] = jnp.zeros(r.fsend.shape, f32)
    r.fbuf[me] = jnp.zeros(r.fsend.shape, f32)
    for copy in [loads[8]] + loads[:8]:
        copy.wait()
    first_f, second_f = r.f_ref[0:2, :], r.f_ref[2:4, :]
    r.fsend[0:2, :] = jnp.where(y == 0, second_f, first_f)
    r.fbuf[me, 0:2, :] = jnp.where(y == 0, first_f, second_f)
    pl.semaphore_wait(barrier, 3 + not_last.astype(jnp.int32) + not_first.astype(jnp.int32))

    def side_moves(block, sources):
        bufs = (r.fbuf, r.kbuf, r.vbuf)
        return [
            remote(a, b.at[block], r.side_send.at[i], r.kv_recv.at[block, i], mate)
            for i, (a, b) in enumerate(zip(sources, bufs))
        ]

    def up_moves(block, target):
        return [
            remote(b.at[block], b.at[block], r.kv_send.at[i], r.kv_recv.at[block, i], target)
            for i, b in enumerate((r.fbuf, r.kbuf, r.vbuf))
        ]

    def pass_up(block):
        @pl.when(not_last)
        def _():
            for copy in up_moves(block, above):
                copy.start()

    def q_move(slot):
        return remote(r.qsend, r.qs.at[slot], r.side_send.at[3], r.q_recv.at[0], mate)

    def parts(refs, quarter, i):
        g, u, d = refs
        tall, flat, wide = g.shape[0] // 4 // PIECES, d.shape[0] // 4, d.shape[1] // PIECES
        span = aligned((quarter * PIECES + i) * tall, tall)
        return (g.at[span, :], u.at[span, :], d.at[aligned(quarter * flat, flat), aligned(i * wide, wide)])

    own_expert = (r.eg.at[0], r.eu.at[0], r.ed.at[0])
    mates_expert = (r.eg.at[1], r.eu.at[1], r.ed.at[1])

    def w_moves(sources, quarter, i, send, recv, target):
        return [
            remote(a, b, send, recv, target)
            for a, b in zip(parts(sources, quarter, i), parts(mates_expert, quarter, i))
        ]

    piece_rows = 3 * (r.eg.shape[1] // 4 // PIECES)

    def w_all(count, send, recv, target):
        one = r.eg.at[1, 0 : count * piece_rows, :]
        return remote(one, one, send, recv, target)

    def w_core_all():
        both = r.eg.at[:, 0 : PIECES * piece_rows, :]
        return remote(both, both, r.wc_sem.at[0], r.wc_sem.at[1], core_mate)

    x_quarter = 2 * (1 - x) + c

    def issue_weights(start, stop):
        def one(i, _):
            for copy in w_moves(own_expert, tp, i, r.wy_send.at[0], r.wy_recv.at[i], mate):
                copy.start()
            return 0

        lax.fori_loop(start, stop, one, 0)

    def issue_extra():
        for i in range(PIECES - EXTRA, PIECES):
            for copy in w_moves(own_expert, x_quarter, i, r.wy_send.at[0], r.wy_recv.at[EXTRA + i], mate):
                copy.start()

    def to_core(i, quarter):
        for copy in w_moves(mates_expert, quarter, i, r.wc_sem.at[0], r.wc_sem.at[1], core_mate):
            copy.start()

    def spread(start, stop):
        def one(i, _):
            w_all(1, r.wy_send.at[0], r.wy_recv.at[i], mate).wait_recv()

            @pl.when(i < PIECES - EXTRA)
            def _():
                for copy in w_moves(mates_expert, tp, i, r.wx_send.at[0], r.wx_recv.at[i], x_mate):
                    copy.start()

            to_core(i, tp)
            return 0

        lax.fori_loop(start, stop, one, 0)

    def spread_x(start, stop):
        def one(i, _):
            w_all(1, r.wx_send.at[0], r.wx_recv.at[i], x_mate).wait_recv()
            to_core(i, x_quarter)
            return 0

        lax.fori_loop(start, stop, one, 0)

    def at_z(*values):
        out = values[-1]
        for level in range(len(values) - 1):
            out = jnp.where(z == level, values[level], out)
        return out

    early = at_z(1, 1, 4, 5)
    for copy in side_moves(me, (r.fsend, r.ksend, r.vsend)):
        copy.start()
    pass_up(me)
    for copy in weights[1:4]:
        copy.start()
    for copy in loads[9:]:
        copy.wait()
    scores = r.score_ref[...]
    gates = scores / jnp.sum(scores, axis=0, keepdims=True) * routed_scale
    for e in range(sp_count):
        r.gbuf[z, e : e + 1, :] = jnp.sum(jnp.where(r.ids_ref[...] == e, gates, 0.0), axis=0, keepdims=True)

    def absorb(i, block, masked):
        q_block = 2 * z + i
        keys, values = r.kbuf[block], r.vbuf[block]
        for j in range(2):
            span = slice(j * q_rows, (j + 1) * q_rows)
            products = lax.dot_general(
                keys, r.qs[i, span, :], (((1,), (1,)), ((), ())), preferred_element_type=f32
            )
            column = jnp.broadcast_to(r.fbuf[block, j : j + 1, :], (HEAD_DIM, q_rows)).T
            column = jnp.concatenate([column] * (q_rows // HEAD_DIM), axis=1)
            drop = r.fbuf[q_block, j : j + 1, :] - column
            part = products * (score_scale * LOG2E) + drop * LOG2E
            if masked:
                at_key = lax.broadcasted_iota(jnp.int32, part.shape, 0)
                at_query = lax.broadcasted_iota(jnp.int32, part.shape, 1)
                part = jnp.where(at_query >= at_key, part, -jnp.inf)
            old = r.top[i, :1, span]
            peak = jnp.maximum(old, jnp.max(part, axis=0, keepdims=True))
            factor = jnp.exp2(old - peak)
            w = jnp.exp2(part - peak)
            r.den[i, :1, span] = r.den[i, :1, span] * factor + jnp.sum(w, axis=0, keepdims=True)
            mixed = lax.dot_general(
                values, w.astype(bf16), (((0,), (0,)), ((), ())), preferred_element_type=f32
            )
            r.acc[i, :, span] = r.acc[i, :, span] * factor + mixed
            r.top[i, :1, span] = peak

    absorb(y, me, True)
    q_move(y).start()
    for copy in weights[1:4]:
        copy.wait()
    issue_weights(0, early)
    for copy in weights[:1] + weights[4:]:
        copy.start()
    def pick(turn, values):
        out = values[-1]
        for k in range(len(values) - 1):
            out = jnp.where(turn == k, values[k], out)
        return out

    def turn_block(turn):
        level = at_z(0, 0, pick(turn, (1, 0, 1, 0)), pick(turn, (2, 1, 2, 0, 1, 0)))
        other = at_z(0, pick(turn, (0, 1)), pick(turn, (0, 0, 1, 1)), pick(turn, (0, 0, 1, 0, 1, 1)))
        return 2 * level + jnp.where(other == 0, y, 1 - y)

    def take_keys(turn):
        block = turn_block(turn)
        for copy in up_moves(block, below):
            copy.wait_recv()
        pass_up(block)

    @pl.when(not_first)
    def _():
        take_keys(0)

    for copy in side_moves(mate_block, (r.fsend, r.ksend, r.vsend)):
        copy.wait_recv()
    pass_up(mate_block)

    @pl.when(not_first)
    def _():
        take_keys(1)

    q_move(1 - y).wait_recv()
    absorb(1 - y, mate_block, True)
    absorb(1, 2 * z, False)

    def take(turn, _):
        ahead = jnp.where(z == last, turn, turn + 1)

        @pl.when(jnp.logical_and(ahead >= 2, ahead < 2 * z))
        def _():
            take_keys(ahead)

        block = turn_block(turn)
        absorb(1 - y, block, False)

        @pl.when(turn < 2 * z - 1)
        def _():
            absorb(y, block, False)

        @pl.when(jnp.logical_and(z == last, jnp.logical_and(turn >= 1, turn < 4)))
        def _():
            spread(turn - 1, turn)

        @pl.when(jnp.logical_and(z == last - 1, jnp.logical_and(turn >= 1, turn < 3)))
        def _():
            spread(turn - 1, turn)

        return 0

    lax.fori_loop(0, 2 * z, take, 0)

    def finish(i, target):
        for j in range(2):
            span = slice(j * q_rows, (j + 1) * q_rows)
            done = (r.acc[i, :, span] / r.den[i, :1, span]).T
            target[:, j * HEAD_DIM : (j + 1) * HEAD_DIM] = done.astype(bf16)

    far, near = (1 - x) * 2, x * 2

    def back_move(slot, i):
        span = aligned((far if i == 0 else near) * rows, 2 * rows)
        return remote(r.attsend.at[span, :], r.att.at[slot, span, :], r.back_send.at[i], r.back_recv.at[i], mate)

    finish(1 - y, r.attsend)
    for i in range(2):
        back_move(y, i).start()
    issue_weights(early, PIECES)
    issue_extra()

    @pl.when(not_first)
    def _():
        absorb(y, 1 - y, False)

    finish(y, r.att.at[y])
    marks = [at_z(0, 0, 2, 3), at_z(1, 1, 3, 4), at_z(2, 2, 5, 6), at_z(4, 4, 6, 8), at_z(6, 6, 7, 8)]
    x_mark = at_z(1, 1, 3, 4)
    spread(marks[0], marks[1])

    weights[0].wait()
    half = r.att.shape[2]

    def core_copy(i):
        return remote(r.core_out.at[i], r.core_in.at[i], r.pair_sem.at[0, i], r.pair_sem.at[1, i], core_mate)

    part_rows = rows // ROW_PIECES

    def piece(ref, p):
        return ref.at[pl.ds(p * part_rows, part_rows), :]

    def hop(p):
        return remote(piece(r.x_out, p), piece(r.x_in, p), r.hop_send.at[0], r.hop_recv.at[p], x_mate)

    def project_to(i, _):
        out_x = jnp.where(i == 0, far, near)
        back = remote(
            r.attsend.at[0 : 2 * rows, :], r.attsend.at[0 : 2 * rows, :], r.back_send.at[i], r.back_recv.at[i], mate
        )
        back.wait_recv()
        span = aligned(out_x * rows, 2 * rows)
        r.pair[...] = jnp.dot(
            r.att[0, span, :], r.wo[0:half, :], preferred_element_type=f32
        ) + jnp.dot(r.att[1, span, :], r.wo[half : 2 * half, :], preferred_element_type=f32)
        r.core_out[i] = r.pair[aligned((1 - c) * rows, rows), :].astype(bf16)
        core_copy(i).start()
        r.kept[i] = r.pair[aligned(c * rows, rows), :]
        return 0

    lax.fori_loop(0, 2, project_to, 0)
    core_copy(0).wait_recv()
    for p in range(ROW_PIECES):
        span = slice(p * part_rows, (p + 1) * part_rows)
        r.x_out[span, :] = (r.kept[0, span, :] + r.core_in[0, span, :].astype(f32)).astype(bf16)
        hop(p).start()
    core_copy(1).wait_recv()
    spread(marks[1], marks[2])

    def tok_move(level, p, send, target):
        return remote(
            piece(r.tok.at[level], p), piece(r.tok.at[level], p), send.at[0], r.tok_recv.at[level, p], target
        )

    def gate_move(level, send, target):
        return remote(r.gbuf.at[level], r.gbuf.at[level], send.at[0], r.gate_recv.at[level], target)

    @pl.when(not_last)
    def _():
        gate_move(z, r.gate_up, above).start()

    @pl.when(not_first)
    def _():
        gate_move(z, r.gate_dn, below).start()

    for p in range(ROW_PIECES):
        span = slice(p * part_rows, (p + 1) * part_rows)
        branch = r.kept[1, span, :] + r.core_in[1, span, :].astype(f32) + r.res_ref[span, :].astype(f32)
        hop(p).wait_recv()
        stream = (branch + r.x_in[span, :].astype(f32)).astype(bf16)
        wide = stream.astype(f32)
        scale = lax.rsqrt(jnp.mean(wide * wide, axis=1, keepdims=True) + norm_eps)
        r.tok[z, span, :] = (wide * scale * r.gain_ref[...]).astype(bf16)
        r.base[span, :] = wide

        @pl.when(not_last)
        def _():
            tok_move(z, p, r.tok_up, above).start()

        @pl.when(not_first)
        def _():
            tok_move(z, p, r.tok_dn, below).start()

    spread(marks[2], marks[3])
    spread_x(0, x_mark)
    for copy in weights[4:]:
        copy.wait()

    def gated(inputs, gate, up, down):
        first = jnp.dot(inputs, gate[...], preferred_element_type=f32)
        second = jnp.dot(inputs, up[...], preferred_element_type=f32)
        hidden = (first / (1.0 + jnp.exp(-first)) * second).astype(bf16)
        return jnp.dot(hidden, down[...], preferred_element_type=f32)

    def expert(level, slot, number):
        table = r.gbuf[level]
        at_expert = lax.broadcasted_iota(jnp.int32, table.shape, 0) == number
        row = jnp.sum(jnp.where(at_expert, table, 0.0), axis=0, keepdims=True)
        shape = (rows, row.shape[1])
        diagonal = lax.broadcasted_iota(jnp.int32, shape, 0) == lax.broadcasted_iota(jnp.int32, shape, 1)
        column = jnp.sum(jnp.where(diagonal, row, 0.0), axis=1, keepdims=True)
        result = gated(r.tok[level], r.eg.at[slot], r.eu.at[slot], r.ed.at[slot])
        return result.astype(bf16).astype(f32) * column

    def arrive_piece(level, p):
        @pl.when(level < z)
        def _():
            if p == 0:
                gate_move(level, r.gate_up, below).wait_recv()
            tok_move(level, p, r.tok_up, below).wait_recv()

            @pl.when(not_last)
            def _():
                if p == 0:
                    gate_move(level, r.gate_up, above).start()
                tok_move(level, p, r.tok_up, above).start()

        @pl.when(level > z)
        def _():
            if p == 0:
                gate_move(level, r.gate_dn, above).wait_recv()
            tok_move(level, p, r.tok_dn, above).wait_recv()

            @pl.when(not_first)
            def _():
                if p == 0:
                    gate_move(level, r.gate_dn, below).start()
                tok_move(level, p, r.tok_dn, below).start()

    def arrive(level):
        for p in range(ROW_PIECES):
            arrive_piece(level, p)

    def up_back(level, p):
        return remote(
            piece(r.ret_out.at[level], p), piece(r.up_in.at[level], p), r.ret_send.at[0], r.up_recv.at[level, p], above
        )

    def dn_back(level, p):
        return remote(
            piece(r.ret_out.at[level], p), piece(r.dn_in.at[level], p), r.ret_send.at[0], r.dn_recv.at[level, p], below
        )

    def give_back(level):
        def send(back, came, chained):
            for p in range(ROW_PIECES):
                span = pl.ds(p * part_rows, part_rows)

                @pl.when(chained)
                def _():
                    back(level, p).wait_recv()
                    r.ret_out[level, span, :] = (
                        r.own[level, span, :] + came[level, span, :].astype(f32)
                    ).astype(bf16)

                @pl.when(jnp.logical_not(chained))
                def _():
                    r.ret_out[level, span, :] = r.own[level, span, :].astype(bf16)

                back(level, p).start()

        @pl.when(level > z)
        def _():
            send(up_back, r.up_in, not_first)

        @pl.when(level < z)
        def _():
            send(dn_back, r.dn_in, not_last)

    def own_expert_on(level):
        r.own[level] = expert(level, 0, me)

    def mates_expert_on(level):
        r.own[level] += expert(level, 1, mate_block)

    def first_turns(k, _):
        level = jnp.where(k == 0, at_z(1, 0, 1, 2), jnp.where(k == 1, at_z(2, 2, 0, 1), z))

        @pl.when(k < 2)
        def _():
            for p in range(ROW_PIECES):
                arrive_piece(level, p)

                @pl.when(jnp.logical_and(z == last - 1, k == 1))
                def _():
                    arrive_piece(last, p)

            spread(jnp.where(k == 0, marks[3], marks[4]), jnp.where(k == 0, marks[4], PIECES))

        own_expert_on(level)
        return 0

    lax.fori_loop(0, 3, first_turns, 0)
    r.base[...] += gated(r.tok[z], r.sg, r.su, r.sd)

    @pl.when(not_first)
    def _():
        level = at_z(0, 3, 3, 0)

        @pl.when(z != last - 1)
        def _():
            arrive(level)

        own_expert_on(level)

    spread_x(x_mark, PIECES - EXTRA)
    for i in range(PIECES - EXTRA, PIECES):
        w_all(1, r.wy_send.at[0], r.wy_recv.at[EXTRA + i], mate).wait_recv()
        to_core(i, x_quarter)
    w_core_all().wait_recv()

    def second_turns(k, _):
        level = jnp.where(k == line - 1, z, at_z(k + 1, pick(k, (3, 0, 2)), pick(k, (0, 3, 1)), k))

        @pl.when(jnp.logical_and(z == 0, k == 2))
        def _():
            arrive(level)
            own_expert_on(level)

        mates_expert_on(level)

        @pl.when(jnp.logical_or(jnp.logical_and(z == last, k < line - 1), jnp.logical_and(z == 0, k == 0)))
        def _():
            give_back(level)

        @pl.when(jnp.logical_and(z == 0, k == 2))
        def _():
            give_back(last)
            give_back(2)

        return 0

    lax.fori_loop(0, line, second_turns, 0)
    r.base[...] += r.own[z]

    @pl.when(jnp.logical_and(not_first, not_last))
    def _():
        def middle(k, _):
            give_back(at_z(0, pick(k, (3, 0, 2)), pick(k, (0, 3, 1)), 0))
            return 0

        lax.fori_loop(0, line - 1, middle, 0)

    @pl.when(not_first)
    def _():
        for p in range(ROW_PIECES):
            up_back(z, p).wait_recv()
        r.base[...] += r.up_in[z].astype(f32)

    @pl.when(not_last)
    def _():
        for p in range(ROW_PIECES):
            dn_back(z, p).wait_recv()
        r.base[...] += r.dn_in[z].astype(f32)

    r.out_ref[...] = r.base[...].astype(bf16)

    for copy in side_moves(me, (r.fsend, r.ksend, r.vsend)) + [q_move(y), back_move(y, 0), back_move(y, 1)]:
        copy.wait_send()
    for i in range(2):
        core_copy(i).wait_send()
    def sent(whole, send, recv, target):
        remote(whole, whole, send, recv, target).wait_send()

    sent(r.x_out, r.hop_send.at[0], r.hop_recv.at[0], x_mate)
    w_all(PIECES + EXTRA, r.wy_send.at[0], r.wy_recv.at[0], mate).wait_send()
    w_all(PIECES - EXTRA, r.wx_send.at[0], r.wx_recv.at[0], x_mate).wait_send()
    w_core_all().wait_send()
    done = pl.ds(0, line - 1)

    @pl.when(not_last)
    def _():
        for level in range(last):

            @pl.when(z == level)
            def _():
                blocks, levels = pl.ds(0, 2 * level + 2), pl.ds(0, level + 1)
                for i, b in enumerate((r.fbuf, r.kbuf, r.vbuf)):
                    sent(b.at[blocks], r.kv_send.at[i], r.kv_recv.at[0, i], above)
                sent(r.gbuf.at[levels], r.gate_up.at[0], r.gate_recv.at[0], above)
                sent(r.tok.at[levels], r.tok_up.at[0], r.tok_recv.at[0, 0], above)

    @pl.when(not_first)
    def _():
        for level in range(1, line):

            @pl.when(z == level)
            def _():
                levels = pl.ds(0, line - level)
                sent(r.gbuf.at[levels], r.gate_dn.at[0], r.gate_recv.at[0], below)
                sent(r.tok.at[levels], r.tok_dn.at[0], r.tok_recv.at[0, 0], below)

    sent(r.ret_out.at[done], r.ret_send.at[0], r.up_recv.at[0, 0], above)


def layer_fused(
    residual,
    queries,
    key_rows,
    value_rows,
    forget_sums,
    norm_gain,
    expert_ids,
    route_weights,
    out_weight,
    expert_gate,
    expert_up,
    expert_down,
    shared_gate,
    shared_up,
    shared_down,
    sp_count,
):
    q_rows, features = queries.shape
    rows, width = residual.shape
    line = sp_count // 2
    bf16, f32 = jnp.bfloat16, jnp.float32
    vmem, hbm = pl.BlockSpec(memory_space=pltpu.VMEM), pl.BlockSpec(memory_space=pl.ANY)
    loaded = (
        out_weight,
        expert_gate[0],
        expert_up[0],
        expert_down[0],
        shared_gate,
        shared_up,
        shared_down,
    )
    ins = ["q_hbm", "f_hbm", "k_hbm", "v_hbm", "res_hbm", "gain_hbm", "ids_hbm", "score_hbm"]
    ins += ["wo_hbm", "eg_hbm", "eu_hbm", "ed_hbm", "sg_hbm", "su_hbm", "sd_hbm"]
    one, per_level = (rows, width), (line, rows, width)
    stacked = (2 * q_rows, HEAD_DIM)

    def buf(*shape):
        return pltpu.VMEM(shape, bf16)

    def wide(*shape):
        return pltpu.VMEM(shape, f32)

    def dma(*shape):
        return pltpu.SemaphoreType.DMA(shape)

    scratch = {
        "qs": buf(2, *stacked),
        "qsend": buf(*stacked),
        "kbuf": buf(sp_count, q_rows, HEAD_DIM),
        "vbuf": buf(sp_count, q_rows, HEAD_DIM),
        "fbuf": wide(sp_count, 8, q_rows),
        "ksend": buf(q_rows, HEAD_DIM),
        "vsend": buf(q_rows, HEAD_DIM),
        "fsend": wide(8, q_rows),
        "acc": wide(2, HEAD_DIM, 2 * q_rows),
        "top": wide(2, 8, 2 * q_rows),
        "den": wide(2, 8, 2 * q_rows),
        "att": buf(2, q_rows, features // 2),
        "attsend": buf(q_rows, features // 2),
        "wo": buf(*out_weight.shape),
        "eg": buf(2, *expert_gate.shape[1:]),
        "eu": buf(2, *expert_up.shape[1:]),
        "ed": buf(2, *expert_down.shape[1:]),
        "sg": buf(*shared_gate.shape),
        "su": buf(*shared_up.shape),
        "sd": buf(*shared_down.shape),
        "gbuf": wide(line, sp_count, rows),
        "pair": wide(2 * rows, width),
        "kept": wide(2, *one),
        "core_out": buf(2, *one),
        "core_in": buf(2, *one),
        "x_out": buf(*one),
        "x_in": buf(*one),
        "base": wide(*one),
        "tok": buf(*per_level),
        "own": wide(*per_level),
        "ret_out": buf(*per_level),
        "up_in": buf(*per_level),
        "dn_in": buf(*per_level),
        "f_ref": wide(*forget_sums.shape[::-1]),
        "res_ref": buf(*one),
        "gain_ref": wide(1, width),
        "ids_ref": pltpu.VMEM(expert_ids.shape[::-1], jnp.int32),
        "score_ref": wide(*route_weights.shape[::-1]),
        "load_sem": dma(13),
        "weight_sem": dma(7),
        "side_send": dma(4),
        "q_recv": dma(1),
        "kv_send": dma(3),
        "kv_recv": dma(sp_count, 3),
        "back_send": dma(2),
        "back_recv": dma(2),
        "wy_send": dma(1),
        "wy_recv": dma(PIECES + EXTRA),
        "wx_send": dma(1),
        "wx_recv": dma(PIECES),
        "wc_sem": dma(2),
        "pair_sem": dma(2, 2),
        "hop_send": dma(1),
        "hop_recv": dma(ROW_PIECES),
        "tok_up": dma(1),
        "tok_dn": dma(1),
        "tok_recv": dma(line, ROW_PIECES),
        "gate_up": dma(1),
        "gate_dn": dma(1),
        "gate_recv": dma(line),
        "ret_send": dma(1),
        "up_recv": dma(line, ROW_PIECES),
        "dn_recv": dma(line, ROW_PIECES),
    }
    names = ins + ["out_ref"] + list(scratch)
    return pl.pallas_call(
        functools.partial(layer_kernel, names, sp_count, HEAD_DIM ** (-0.5)),
        out_shape=jax.ShapeDtypeStruct(one, bf16),
        in_specs=[hbm] * 15,
        out_specs=vmem,
        scratch_shapes=list(scratch.values()),
        compiler_params=pltpu.CompilerParams(
            collective_id=0, has_side_effects=True, vmem_limit_bytes=60 * 2**20
        ),
    )(
        queries,
        forget_sums.T,
        key_rows,
        value_rows,
        residual,
        norm_gain[None, :],
        expert_ids.T,
        route_weights.T,
        *loaded,
    )


def absorb_group(carried, query_group, shard_piece, sum_piece, score_scale):
    query_heads, query_sums, query_pos, last_pos = query_group
    key_piece, value_piece = shard_piece
    piece_rows = key_piece.shape[0]
    query_count, local_kv, group_size, head_size = query_heads.shape
    key_block = math.gcd(piece_rows, 1024)
    key_heads = key_piece.reshape(piece_rows, local_kv, head_size)
    value_heads = value_piece.reshape(piece_rows, local_kv, head_size)
    key_sums = sum_piece.reshape(piece_rows, local_kv, group_size).transpose(1, 2, 0)

    def update(block_start, held):
        row_max, row_sum, weighted = held
        key_part = lax.dynamic_slice_in_dim(key_heads, block_start, key_block, 0)
        value_part = lax.dynamic_slice_in_dim(value_heads, block_start, key_block, 0)
        sums_part = lax.dynamic_slice_in_dim(key_sums, block_start, key_block, 2)
        scores = (
            jnp.einsum("qhgd,khd->hgqk", query_heads, key_part, preferred_element_type=jnp.float32)
            * score_scale
        )
        scores = scores + (query_sums[:, :, :, None] - sums_part[:, :, None, :])
        key_pos = block_start + jnp.arange(key_block, dtype=jnp.int32)
        allowed = query_pos[:, None] >= key_pos[None, :]
        scores = jnp.where(allowed, scores, -jnp.inf)
        new_max = jnp.maximum(row_max, jnp.max(scores, axis=3))
        weights = jnp.exp(scores - new_max[:, :, :, None])
        factor = jnp.exp(row_max - new_max)
        row_sum = row_sum * factor + jnp.sum(weights, axis=3)
        products = jnp.einsum(
            "hgqk,khd->qhgd",
            weights.astype(jnp.bfloat16),
            value_part,
            preferred_element_type=jnp.float32,
        )
        weighted = weighted * factor.transpose(2, 0, 1)[:, :, :, None] + products
        return (new_max, row_sum, weighted)

    def one_block(block_index, held):
        block_start = block_index * key_block
        needed = block_start <= last_pos
        return lax.cond(needed, lambda inner: update(block_start, inner), lambda inner: inner, held)

    return lax.fori_loop(0, piece_rows // key_block, one_block, carried)


def finish(carried):
    row_max, row_sum, weighted = carried
    mixed = weighted / row_sum.transpose(2, 0, 1)[:, :, :, None]
    return mixed.reshape(mixed.shape[0], -1).astype(jnp.bfloat16)


def local(
    residual,
    queries,
    key_rows,
    value_rows,
    forget_sums,
    out_weight,
    norm_gain,
    expert_ids,
    route_weights,
    expert_gate,
    expert_up,
    expert_down,
    shared_gate,
    shared_up,
    shared_down,
):
    sp_count = lax.axis_size("sp")
    sp_index = lax.axis_index("sp")
    local_rows = queries.shape[0]
    local_kv = key_rows.shape[1] // HEAD_DIM
    group_size = HEADS // KV_HEADS
    score_scale = HEAD_DIM ** (-0.5)
    tp_count = lax.axis_size("tp")
    tokens_here = residual.shape[0]
    every_slot = 2 * tokens_here * TOPK >= tokens_here * expert_gate.shape[0] * sp_count
    if every_slot and expert_gate.shape[0] == 1 and sp_count == 8 and tp_count == 4:
        return layer_fused(
            residual,
            queries,
            key_rows,
            value_rows,
            forget_sums,
            norm_gain,
            expert_ids,
            route_weights,
            out_weight,
            expert_gate,
            expert_up,
            expert_down,
            shared_gate,
            shared_up,
            shared_down,
            sp_count,
        )
    own_first = sp_index * local_rows
    all_sums = lax.all_gather(forget_sums, "sp", axis=0, tiled=True)
    positions = own_first + jnp.arange(local_rows, dtype=jnp.int32)
    groups = [
        (
            queries.reshape(queries.shape[0], local_kv, group_size, HEAD_DIM),
            forget_sums.reshape(forget_sums.shape[0], local_kv, group_size).transpose(1, 2, 0),
            positions,
            positions[-1],
        )
    ]

    def initial(query_count):
        return (
            jnp.full((local_kv, group_size, query_count), -1e30, jnp.float32),
            jnp.zeros((local_kv, group_size, query_count), jnp.float32),
            jnp.zeros((query_count, local_kv, group_size, HEAD_DIM), jnp.float32),
        )

    def absorb(states, shard_piece):
        return tuple(
            (
                absorb_group(held, query_group, shard_piece, all_sums, score_scale)
                for held, query_group in zip(states, groups)
            )
        )

    start_states = tuple((initial(query_group[0].shape[0]) for query_group in groups))
    states = absorb(
        start_states,
        (
            lax.all_gather(key_rows, "sp", axis=0, tiled=True),
            lax.all_gather(value_rows, "sp", axis=0, tiled=True),
        ),
    )
    outputs = [finish(held) for held in states]
    attended = outputs[0]
    rows_out = local_rows // lax.axis_size("tp")
    branch = lax.psum_scatter(
        jnp.dot(attended, out_weight, preferred_element_type=jnp.float32).astype(jnp.bfloat16),
        "tp",
        scatter_dimension=0,
        tiled=True,
    ).astype(jnp.float32)
    stream = (residual.astype(jnp.float32) + branch).astype(jnp.bfloat16)
    wide = lax.optimization_barrier(stream).astype(jnp.float32)
    normed = (
        wide * lax.rsqrt(jnp.mean(wide * wide, axis=1, keepdims=True) + norm_eps) * norm_gain
    ).astype(jnp.bfloat16)
    width = normed.shape[1]
    experts_here = expert_gate.shape[0]
    total_experts = experts_here * sp_count
    capacity = 2 * rows_out * TOPK // total_experts
    flat_ids = expert_ids.reshape(-1)
    assigned = flat_ids.shape[0]
    onehot = (flat_ids[:, None] == jnp.arange(total_experts, dtype=jnp.int32)[None, :]).astype(
        jnp.int32
    )
    slot_rank = jnp.sum((jnp.cumsum(onehot, axis=0) - 1) * onehot, axis=1)
    target = flat_ids * capacity + slot_rank
    slot_count = total_experts * capacity
    source = (
        jnp.full((slot_count,), assigned, jnp.int32)
        .at[target]
        .set(jnp.arange(assigned, dtype=jnp.int32))
    )
    padded = jnp.concatenate([normed, jnp.zeros((1, width), jnp.bfloat16)], axis=0)
    outgoing = padded[source // TOPK].reshape(sp_count, experts_here, capacity, width)
    arrived = lax.all_to_all(outgoing, "sp", split_axis=0, concat_axis=0, tiled=True)
    gate_part = jnp.einsum(
        "necd,edf->necf", arrived, expert_gate, preferred_element_type=jnp.float32
    )
    up_part = jnp.einsum("necd,edf->necf", arrived, expert_up, preferred_element_type=jnp.float32)
    hidden = (jax.nn.silu(gate_part) * up_part).astype(jnp.bfloat16)
    processed = jnp.einsum(
        "necf,efd->necd", hidden, expert_down, preferred_element_type=jnp.float32
    ).astype(jnp.bfloat16)
    returned = lax.all_to_all(processed, "sp", split_axis=0, concat_axis=0, tiled=True)
    results = returned.reshape(slot_count, width)
    picked = results[target].reshape(rows_out, TOPK, width).astype(jnp.float32)
    gates = route_weights / jnp.sum(route_weights, axis=1, keepdims=True) * routed_scale
    routed = jnp.sum(gates[:, :, None] * picked, axis=1)
    shared_hidden = (
        jax.nn.silu(jnp.dot(normed, shared_gate, preferred_element_type=jnp.float32))
        * jnp.dot(normed, shared_up, preferred_element_type=jnp.float32)
    ).astype(jnp.bfloat16)
    shared_out = jnp.dot(shared_hidden, shared_down, preferred_element_type=jnp.float32)
    return (wide + shared_out + routed).astype(jnp.bfloat16)


def solution(mesh):
    in_specs = (
        P(("sp", "tp"), None),
        P("sp", "tp"),
        P("sp", "tp"),
        P("sp", "tp"),
        P("sp", "tp"),
        P("tp", None),
        P(),
        P(("sp", "tp"), None),
        P(("sp", "tp"), None),
        P("sp", None, None),
        P("sp", None, None),
        P("sp", None, None),
        P(),
        P(),
        P(),
    )
    out_specs = P(("sp", "tp"), None)
    return jax.shard_map(local, mesh=mesh, in_specs=in_specs, out_specs=out_specs, check_vma=False)
```

```python
import functools
import math
import types

import jax
import jax.numpy as jnp
from jax import lax
from jax.experimental import pallas as pl
from jax.experimental.pallas import tpu as pltpu
from jax.sharding import PartitionSpec as P

HEADS = 16
KV_HEADS = 8
HEAD_DIM = 128
TOPK = 4


routed_scale = 2.5
norm_eps = 1e-06


MESH_ID = pl.DeviceIdType.MESH
LOG2E = math.log2(math.e)


def remote(src, dst, send_sem, recv_sem, target):
    return pltpu.make_async_remote_copy(
        src_ref=src,
        dst_ref=dst,
        send_sem=send_sem,
        recv_sem=recv_sem,
        device_id=target,
        device_id_type=MESH_ID,
    )


def greet(barrier, target):
    pl.semaphore_signal(barrier, inc=1, device_id=target, device_id_type=MESH_ID)


PIECES = 8
EXTRA = 1
ROW_PIECES = 4


def aligned(start, size):
    return pl.ds(pl.multiple_of(start, size), size)


def layer_kernel(names, sp_count, score_scale, *refs):
    r = types.SimpleNamespace(**dict(zip(names, refs)))
    me, tp = lax.axis_index("sp"), lax.axis_index("tp")
    line = sp_count // 2
    last = line - 1
    z, y = me // 2, me % 2
    x, c = tp // 2, tp % 2
    mate_block = 2 * z + 1 - y
    mate = (mate_block, tp)
    above = (jnp.minimum(me + 2, sp_count - 1), tp)
    below = (jnp.maximum(me - 2, 0), tp)
    core_mate = (me, 2 * x + 1 - c)
    x_mate = (me, 2 * (1 - x) + c)
    not_last, not_first = z < last, z > 0
    q_rows = r.q_hbm.shape[0]
    rows, width = r.res_hbm.shape
    f32, bf16 = jnp.float32, jnp.bfloat16

    barrier = pltpu.get_barrier_semaphore()
    for peer in (mate, core_mate, x_mate):
        greet(barrier, peer)

    @pl.when(not_last)
    def _():
        greet(barrier, above)

    @pl.when(not_first)
    def _():
        greet(barrier, below)

    def lanes(ref, head):
        return ref.at[:, aligned(head * HEAD_DIM, HEAD_DIM)]

    def q_part(ref, j):
        return ref.at[pl.ds(j * q_rows, q_rows), :]

    loads = [
        (lanes(r.k_hbm, 1 - y), r.ksend),
        (lanes(r.v_hbm, 1 - y), r.vsend),
        (lanes(r.k_hbm, y), r.kbuf.at[me]),
        (lanes(r.v_hbm, y), r.vbuf.at[me]),
        (lanes(r.q_hbm, 2 * (1 - y)), q_part(r.qsend, 0)),
        (lanes(r.q_hbm, 2 * (1 - y) + 1), q_part(r.qsend, 1)),
        (lanes(r.q_hbm, 2 * y), q_part(r.qs.at[y], 0)),
        (lanes(r.q_hbm, 2 * y + 1), q_part(r.qs.at[y], 1)),
        (r.f_hbm, r.f_ref),
        (r.ids_hbm, r.ids_ref),
        (r.score_hbm, r.score_ref),
        (r.res_hbm, r.res_ref),
        (r.gain_hbm, r.gain_ref),
    ]
    loads = [pltpu.make_async_copy(a, b, r.load_sem.at[i]) for i, (a, b) in enumerate(loads)]
    for copy in loads:
        copy.start()
    sources = (r.wo_hbm, r.eg_hbm, r.eu_hbm, r.ed_hbm, r.sg_hbm, r.su_hbm, r.sd_hbm)
    held = (r.wo, r.eg.at[0], r.eu.at[0], r.ed.at[0], r.sg, r.su, r.sd)
    weights = [pltpu.make_async_copy(a, b, r.weight_sem.at[i]) for i, (a, b) in enumerate(zip(sources, held))]
    r.acc[...] = jnp.zeros(r.acc.shape, f32)
    r.den[...] = jnp.zeros(r.den.shape, f32)
    r.top[...] = jnp.full(r.top.shape, -jnp.inf, f32)
    r.fsend[...] = jnp.zeros(r.fsend.shape, f32)
    r.fbuf[me] = jnp.zeros(r.fsend.shape, f32)
    for copy in [loads[8]] + loads[:8]:
        copy.wait()
    first_f, second_f = r.f_ref[0:2, :], r.f_ref[2:4, :]
    r.fsend[0:2, :] = jnp.where(y == 0, second_f, first_f)
    r.fbuf[me, 0:2, :] = jnp.where(y == 0, first_f, second_f)
    pl.semaphore_wait(barrier, 3 + not_last.astype(jnp.int32) + not_first.astype(jnp.int32))

    def side_moves(block, sources):
        bufs = (r.fbuf, r.kbuf, r.vbuf)
        return [
            remote(a, b.at[block], r.side_send.at[i], r.kv_recv.at[block, i], mate)
            for i, (a, b) in enumerate(zip(sources, bufs))
        ]

    def up_moves(block, target):
        return [
            remote(b.at[block], b.at[block], r.kv_send.at[i], r.kv_recv.at[block, i], target)
            for i, b in enumerate((r.fbuf, r.kbuf, r.vbuf))
        ]

    def pass_up(block):
        @pl.when(not_last)
        def _():
            for copy in up_moves(block, above):
                copy.start()

    def q_move(slot):
        return remote(r.qsend, r.qs.at[slot], r.side_send.at[3], r.q_recv.at[0], mate)

    def parts(refs, quarter, i):
        g, u, d = refs
        tall, flat, wide = g.shape[0] // 4 // PIECES, d.shape[0] // 4, d.shape[1] // PIECES
        span = aligned((quarter * PIECES + i) * tall, tall)
        return (g.at[span, :], u.at[span, :], d.at[aligned(quarter * flat, flat), aligned(i * wide, wide)])

    own_expert = (r.eg.at[0], r.eu.at[0], r.ed.at[0])
    mates_expert = (r.eg.at[1], r.eu.at[1], r.ed.at[1])

    def w_moves(sources, quarter, i, send, recv, target):
        return [
            remote(a, b, send, recv, target)
            for a, b in zip(parts(sources, quarter, i), parts(mates_expert, quarter, i))
        ]

    piece_rows = 3 * (r.eg.shape[1] // 4 // PIECES)

    def w_all(count, send, recv, target):
        one = r.eg.at[1, 0 : count * piece_rows, :]
        return remote(one, one, send, recv, target)

    def w_core_all():
        both = r.eg.at[:, 0 : PIECES * piece_rows, :]
        return remote(both, both, r.wc_sem.at[0], r.wc_sem.at[1], core_mate)

    x_quarter = 2 * (1 - x) + c

    def issue_weights(start, stop):
        def one(i, _):
            for copy in w_moves(own_expert, tp, i, r.wy_send.at[0], r.wy_recv.at[i], mate):
                copy.start()
            return 0

        lax.fori_loop(start, stop, one, 0)

    def issue_extra():
        for i in range(PIECES - EXTRA, PIECES):
            for copy in w_moves(own_expert, x_quarter, i, r.wy_send.at[0], r.wy_recv.at[EXTRA + i], mate):
                copy.start()

    def to_core(i, quarter):
        for copy in w_moves(mates_expert, quarter, i, r.wc_sem.at[0], r.wc_sem.at[1], core_mate):
            copy.start()

    def spread(start, stop):
        def one(i, _):
            w_all(1, r.wy_send.at[0], r.wy_recv.at[i], mate).wait_recv()

            @pl.when(i < PIECES - EXTRA)
            def _():
                for copy in w_moves(mates_expert, tp, i, r.wx_send.at[0], r.wx_recv.at[i], x_mate):
                    copy.start()

            to_core(i, tp)
            return 0

        lax.fori_loop(start, stop, one, 0)

    def spread_x(start, stop):
        def one(i, _):
            w_all(1, r.wx_send.at[0], r.wx_recv.at[i], x_mate).wait_recv()
            to_core(i, x_quarter)
            return 0

        lax.fori_loop(start, stop, one, 0)

    def at_z(*values):
        out = values[-1]
        for level in range(len(values) - 1):
            out = jnp.where(z == level, values[level], out)
        return out

    early = at_z(1, 2, 3, 5)
    for copy in side_moves(me, (r.fsend, r.ksend, r.vsend)):
        copy.start()
    pass_up(me)
    for copy in weights[1:4]:
        copy.start()
    for copy in loads[9:]:
        copy.wait()
    scores = r.score_ref[...]
    gates = scores / jnp.sum(scores, axis=0, keepdims=True) * routed_scale
    for e in range(sp_count):
        r.gbuf[z, e : e + 1, :] = jnp.sum(jnp.where(r.ids_ref[...] == e, gates, 0.0), axis=0, keepdims=True)

    def absorb(i, block, masked):
        q_block = 2 * z + i
        keys, values = r.kbuf[block], r.vbuf[block]
        for j in range(2):
            span = slice(j * q_rows, (j + 1) * q_rows)
            products = lax.dot_general(
                keys, r.qs[i, span, :], (((1,), (1,)), ((), ())), preferred_element_type=f32
            )
            column = jnp.broadcast_to(r.fbuf[block, j : j + 1, :], (HEAD_DIM, q_rows)).T
            column = jnp.concatenate([column] * (q_rows // HEAD_DIM), axis=1)
            drop = r.fbuf[q_block, j : j + 1, :] - column
            part = products * (score_scale * LOG2E) + drop * LOG2E
            if masked:
                at_key = lax.broadcasted_iota(jnp.int32, part.shape, 0)
                at_query = lax.broadcasted_iota(jnp.int32, part.shape, 1)
                part = jnp.where(at_query >= at_key, part, -jnp.inf)
            old = r.top[i, :1, span]
            peak = jnp.maximum(old, jnp.max(part, axis=0, keepdims=True))
            factor = jnp.exp2(old - peak)
            w = jnp.exp2(part - peak)
            r.den[i, :1, span] = r.den[i, :1, span] * factor + jnp.sum(w, axis=0, keepdims=True)
            mixed = lax.dot_general(
                values, w.astype(bf16), (((0,), (0,)), ((), ())), preferred_element_type=f32
            )
            r.acc[i, :, span] = r.acc[i, :, span] * factor + mixed
            r.top[i, :1, span] = peak

    absorb(y, me, True)
    q_move(y).start()
    for copy in weights[1:4]:
        copy.wait()
    issue_weights(0, early)
    for copy in weights[:1] + weights[4:]:
        copy.start()
    def pick(turn, values):
        out = values[-1]
        for k in range(len(values) - 1):
            out = jnp.where(turn == k, values[k], out)
        return out

    def turn_block(turn):
        level = at_z(0, 0, pick(turn, (1, 0, 1, 0)), pick(turn, (2, 1, 2, 0, 1, 0)))
        other = at_z(0, pick(turn, (0, 1)), pick(turn, (0, 0, 1, 1)), pick(turn, (0, 0, 1, 0, 1, 1)))
        return 2 * level + jnp.where(other == 0, y, 1 - y)

    def take_keys(turn):
        block = turn_block(turn)
        for copy in up_moves(block, below):
            copy.wait_recv()
        pass_up(block)

    @pl.when(not_first)
    def _():
        take_keys(0)

    for copy in side_moves(mate_block, (r.fsend, r.ksend, r.vsend)):
        copy.wait_recv()
    pass_up(mate_block)

    @pl.when(not_first)
    def _():
        take_keys(1)

    q_move(1 - y).wait_recv()
    absorb(1 - y, mate_block, True)
    absorb(1, 2 * z, False)

    def take(turn, _):
        ahead = jnp.where(z == last, turn, turn + 1)

        @pl.when(jnp.logical_and(ahead >= 2, ahead < 2 * z))
        def _():
            take_keys(ahead)

        block = turn_block(turn)
        absorb(1 - y, block, False)

        @pl.when(turn < 2 * z - 1)
        def _():
            absorb(y, block, False)

        @pl.when(turn == 0)
        def _():
            spread(0, 1)

        @pl.when(jnp.logical_and(z >= last - 1, turn == 2))
        def _():
            spread(1, 2)

        @pl.when(jnp.logical_and(z == last, turn == 3))
        def _():
            spread(2, 3)

        return 0

    lax.fori_loop(0, 2 * z, take, 0)

    def finish(i, target):
        for j in range(2):
            span = slice(j * q_rows, (j + 1) * q_rows)
            done = (r.acc[i, :, span] / r.den[i, :1, span]).T
            target[:, j * HEAD_DIM : (j + 1) * HEAD_DIM] = done.astype(bf16)

    far, near = (1 - x) * 2, x * 2

    def back_move(slot, i):
        span = aligned((far if i == 0 else near) * rows, 2 * rows)
        return remote(r.attsend.at[span, :], r.att.at[slot, span, :], r.back_send.at[i], r.back_recv.at[i], mate)

    finish(1 - y, r.attsend)
    for i in range(2):
        back_move(y, i).start()
    issue_weights(early, PIECES)
    issue_extra()

    @pl.when(not_first)
    def _():
        absorb(y, 1 - y, False)

    finish(y, r.att.at[y])
    marks = [at_z(0, 1, 2, 3), at_z(1, 2, 3, 5), at_z(2, 3, 4, 6), at_z(6, 4, 6, 7), at_z(8, 6, 7, 8), at_z(8, 7, 8, 8)]
    x_mark = at_z(1, 2, 3, 4)
    spread(marks[0], marks[1])

    weights[0].wait()
    half = r.att.shape[2]

    def core_copy(i):
        return remote(r.core_out.at[i], r.core_in.at[i], r.pair_sem.at[0, i], r.pair_sem.at[1, i], core_mate)

    part_rows = rows // ROW_PIECES

    def piece(ref, p):
        return ref.at[pl.ds(p * part_rows, part_rows), :]

    def hop(p):
        return remote(piece(r.x_out, p), piece(r.x_in, p), r.hop_send.at[0], r.hop_recv.at[p], x_mate)

    def project_to(i, _):
        out_x = jnp.where(i == 0, far, near)
        back = remote(
            r.attsend.at[0 : 2 * rows, :], r.attsend.at[0 : 2 * rows, :], r.back_send.at[i], r.back_recv.at[i], mate
        )
        back.wait_recv()
        span = aligned(out_x * rows, 2 * rows)
        r.pair[...] = jnp.dot(
            r.att[0, span, :], r.wo[0:half, :], preferred_element_type=f32
        ) + jnp.dot(r.att[1, span, :], r.wo[half : 2 * half, :], preferred_element_type=f32)
        r.core_out[i] = r.pair[aligned((1 - c) * rows, rows), :].astype(bf16)
        core_copy(i).start()
        r.kept[i] = r.pair[aligned(c * rows, rows), :]
        return 0

    lax.fori_loop(0, 2, project_to, 0)
    core_copy(0).wait_recv()
    for p in range(ROW_PIECES):
        span = slice(p * part_rows, (p + 1) * part_rows)
        r.x_out[span, :] = (r.kept[0, span, :] + r.core_in[0, span, :].astype(f32)).astype(bf16)
        hop(p).start()
    core_copy(1).wait_recv()
    spread(marks[1], marks[2])

    def tok_move(level, p, send, target):
        return remote(
            piece(r.tok.at[level], p), piece(r.tok.at[level], p), send.at[0], r.tok_recv.at[level, p], target
        )

    def gate_move(level, send, target):
        return remote(r.gbuf.at[level], r.gbuf.at[level], send.at[0], r.gate_recv.at[level], target)

    def arrive_piece(level, p):
        @pl.when(level < z)
        def _():
            if p == 0:
                gate_move(level, r.gate_up, below).wait_recv()
            tok_move(level, p, r.tok_up, below).wait_recv()

            @pl.when(not_last)
            def _():
                if p == 0:
                    gate_move(level, r.gate_up, above).start()
                tok_move(level, p, r.tok_up, above).start()

        @pl.when(level > z)
        def _():
            if p == 0:
                gate_move(level, r.gate_dn, above).wait_recv()
            tok_move(level, p, r.tok_dn, above).wait_recv()

            @pl.when(not_first)
            def _():
                if p == 0:
                    gate_move(level, r.gate_dn, below).start()
                tok_move(level, p, r.tok_dn, below).start()

    def arrive(level):
        for p in range(ROW_PIECES):
            arrive_piece(level, p)

    @pl.when(not_last)
    def _():
        gate_move(z, r.gate_up, above).start()

    @pl.when(not_first)
    def _():
        gate_move(z, r.gate_dn, below).start()

    for p in range(ROW_PIECES):
        span = slice(p * part_rows, (p + 1) * part_rows)
        branch = r.kept[1, span, :] + r.core_in[1, span, :].astype(f32) + r.res_ref[span, :].astype(f32)
        hop(p).wait_recv()
        stream = (branch + r.x_in[span, :].astype(f32)).astype(bf16)
        wide = stream.astype(f32)
        scale = lax.rsqrt(jnp.mean(wide * wide, axis=1, keepdims=True) + norm_eps)
        r.tok[z, span, :] = (wide * scale * r.gain_ref[...]).astype(bf16)
        r.base[span, :] = wide

        @pl.when(z == 1)
        def _():
            arrive_piece(0, p)

        @pl.when(not_last)
        def _():
            tok_move(z, p, r.tok_up, above).start()

        @pl.when(not_first)
        def _():
            tok_move(z, p, r.tok_dn, below).start()

    spread(marks[2], marks[3])
    spread_x(0, x_mark)
    for copy in weights[4:]:
        copy.wait()

    def gated(inputs, gate, up, down):
        first = jnp.dot(inputs, gate[...], preferred_element_type=f32)
        second = jnp.dot(inputs, up[...], preferred_element_type=f32)
        hidden = (first / (1.0 + jnp.exp(-first)) * second).astype(bf16)
        return jnp.dot(hidden, down[...], preferred_element_type=f32)

    def expert(level, slot, number):
        table = r.gbuf[level]
        at_expert = lax.broadcasted_iota(jnp.int32, table.shape, 0) == number
        row = jnp.sum(jnp.where(at_expert, table, 0.0), axis=0, keepdims=True)
        shape = (rows, row.shape[1])
        diagonal = lax.broadcasted_iota(jnp.int32, shape, 0) == lax.broadcasted_iota(jnp.int32, shape, 1)
        column = jnp.sum(jnp.where(diagonal, row, 0.0), axis=1, keepdims=True)
        result = gated(r.tok[level], r.eg.at[slot], r.eu.at[slot], r.ed.at[slot])
        return result.astype(bf16).astype(f32) * column

    def up_back(level, p):
        return remote(
            piece(r.ret_out.at[level], p), piece(r.up_in.at[level], p), r.ret_send.at[0], r.up_recv.at[level, p], above
        )

    def dn_back(level, p):
        return remote(
            piece(r.ret_out.at[level], p), piece(r.dn_in.at[level], p), r.ret_send.at[0], r.dn_recv.at[level, p], below
        )

    def give_piece(level, p):
        span = pl.ds(p * part_rows, part_rows)

        def send(back, came, chained):
            @pl.when(chained)
            def _():
                back(level, p).wait_recv()
                r.ret_out[level, span, :] = (r.own[level, span, :] + came[level, span, :].astype(f32)).astype(bf16)

            @pl.when(jnp.logical_not(chained))
            def _():
                r.ret_out[level, span, :] = r.own[level, span, :].astype(bf16)

            back(level, p).start()

        @pl.when(level > z)
        def _():
            send(up_back, r.up_in, not_first)

        @pl.when(level < z)
        def _():
            send(dn_back, r.dn_in, not_last)

    def give_back(level):
        for p in range(ROW_PIECES):
            give_piece(level, p)

    def own_expert_on(level):
        r.own[level] = expert(level, 0, me)

    def mates_expert_on(level):
        r.own[level] += expert(level, 1, mate_block)

    def first_turns(k, _):
        level = jnp.where(k == 0, at_z(1, 0, 0, 2), jnp.where(k == 1, at_z(2, 2, 1, 0), z))

        @pl.when(k < 2)
        def _():
            for p in range(ROW_PIECES):

                @pl.when(jnp.logical_or(z != 1, k == 1))
                def _():
                    arrive_piece(level, p)

                @pl.when(jnp.logical_and(z == last - 1, k == 1))
                def _():
                    arrive_piece(last, p)

            spread(jnp.where(k == 0, marks[3], marks[4]), jnp.where(k == 0, marks[4], marks[5]))

        own_expert_on(level)
        return 0

    lax.fori_loop(0, 3, first_turns, 0)
    r.base[...] += gated(r.tok[z], r.sg, r.su, r.sd)
    spread(marks[5], PIECES)

    @pl.when(jnp.logical_and(not_first, not_last))
    def _():
        @pl.when(z == 1)
        def _():
            arrive(last)

        own_expert_on(last)

    spread_x(x_mark, PIECES - EXTRA)
    for i in range(PIECES - EXTRA, PIECES):
        w_all(1, r.wy_send.at[0], r.wy_recv.at[EXTRA + i], mate).wait_recv()
        to_core(i, x_quarter)
    w_core_all().wait_recv()

    def second_turns(k, _):
        level = at_z(pick(k, (2, 1, 3)), pick(k, (2, 0, 3)), pick(k, (0, 1, 3)), k)

        @pl.when(jnp.logical_or(jnp.logical_and(z == 0, k == 2), jnp.logical_and(z == last, k == 1)))
        def _():
            arrive(level)
            own_expert_on(level)

        mates_expert_on(level)

        @pl.when(jnp.logical_or(z == last, jnp.logical_and(z == 0, k != 1)))
        def _():
            give_back(level)

        return 0

    lax.fori_loop(0, line - 1, second_turns, 0)

    give_back(at_z(1, 2, 0, z))
    mates_expert_on(z)
    r.base[...] += r.own[z]

    @pl.when(jnp.logical_and(not_first, not_last))
    def _():
        lag = 2
        for step in range(ROW_PIECES + lag):

            @pl.when(z == 1)
            def _():
                if step < ROW_PIECES:
                    give_piece(0, step)
                    give_piece(last, step)

            @pl.when(z == last - 1)
            def _():
                if step < ROW_PIECES:
                    give_piece(1, step)
                if step >= lag:
                    give_piece(last, step - lag)

    for p in range(ROW_PIECES):
        span = slice(p * part_rows, (p + 1) * part_rows)

        @pl.when(not_first)
        def _():
            up_back(z, p).wait_recv()
            r.base[span, :] += r.up_in[z, span, :].astype(f32)

        @pl.when(not_last)
        def _():
            dn_back(z, p).wait_recv()
            r.base[span, :] += r.dn_in[z, span, :].astype(f32)

        r.out_ref[span, :] = r.base[span, :].astype(bf16)

    for copy in side_moves(me, (r.fsend, r.ksend, r.vsend)) + [q_move(y), back_move(y, 0), back_move(y, 1)]:
        copy.wait_send()
    for i in range(2):
        core_copy(i).wait_send()
    def sent(whole, send, recv, target):
        remote(whole, whole, send, recv, target).wait_send()

    sent(r.x_out, r.hop_send.at[0], r.hop_recv.at[0], x_mate)
    w_all(PIECES + EXTRA, r.wy_send.at[0], r.wy_recv.at[0], mate).wait_send()
    w_all(PIECES - EXTRA, r.wx_send.at[0], r.wx_recv.at[0], x_mate).wait_send()
    w_core_all().wait_send()
    done = pl.ds(0, line - 1)

    @pl.when(not_last)
    def _():
        for level in range(last):

            @pl.when(z == level)
            def _():
                blocks, levels = pl.ds(0, 2 * level + 2), pl.ds(0, level + 1)
                for i, b in enumerate((r.fbuf, r.kbuf, r.vbuf)):
                    sent(b.at[blocks], r.kv_send.at[i], r.kv_recv.at[0, i], above)
                sent(r.gbuf.at[levels], r.gate_up.at[0], r.gate_recv.at[0], above)
                sent(r.tok.at[levels], r.tok_up.at[0], r.tok_recv.at[0, 0], above)

    @pl.when(not_first)
    def _():
        for level in range(1, line):

            @pl.when(z == level)
            def _():
                levels = pl.ds(0, line - level)
                sent(r.gbuf.at[levels], r.gate_dn.at[0], r.gate_recv.at[0], below)
                sent(r.tok.at[levels], r.tok_dn.at[0], r.tok_recv.at[0, 0], below)

    sent(r.ret_out.at[done], r.ret_send.at[0], r.up_recv.at[0, 0], above)


def layer_fused(
    residual,
    queries,
    key_rows,
    value_rows,
    forget_sums,
    norm_gain,
    expert_ids,
    route_weights,
    out_weight,
    expert_gate,
    expert_up,
    expert_down,
    shared_gate,
    shared_up,
    shared_down,
    sp_count,
):
    q_rows, features = queries.shape
    rows, width = residual.shape
    line = sp_count // 2
    bf16, f32 = jnp.bfloat16, jnp.float32
    hbm = pl.BlockSpec(memory_space=pl.ANY)
    loaded = (
        out_weight,
        expert_gate[0],
        expert_up[0],
        expert_down[0],
        shared_gate,
        shared_up,
        shared_down,
    )
    ins = ["q_hbm", "f_hbm", "k_hbm", "v_hbm", "res_hbm", "gain_hbm", "ids_hbm", "score_hbm"]
    ins += ["wo_hbm", "eg_hbm", "eu_hbm", "ed_hbm", "sg_hbm", "su_hbm", "sd_hbm"]
    one, per_level = (rows, width), (line, rows, width)
    stacked = (2 * q_rows, HEAD_DIM)

    def buf(*shape):
        return pltpu.VMEM(shape, bf16)

    def wide(*shape):
        return pltpu.VMEM(shape, f32)

    def dma(*shape):
        return pltpu.SemaphoreType.DMA(shape)

    scratch = {
        "qs": buf(2, *stacked),
        "qsend": buf(*stacked),
        "kbuf": buf(sp_count, q_rows, HEAD_DIM),
        "vbuf": buf(sp_count, q_rows, HEAD_DIM),
        "fbuf": wide(sp_count, 8, q_rows),
        "ksend": buf(q_rows, HEAD_DIM),
        "vsend": buf(q_rows, HEAD_DIM),
        "fsend": wide(8, q_rows),
        "acc": wide(2, HEAD_DIM, 2 * q_rows),
        "top": wide(2, 8, 2 * q_rows),
        "den": wide(2, 8, 2 * q_rows),
        "att": buf(2, q_rows, features // 2),
        "attsend": buf(q_rows, features // 2),
        "wo": buf(*out_weight.shape),
        "eg": buf(2, *expert_gate.shape[1:]),
        "eu": buf(2, *expert_up.shape[1:]),
        "ed": buf(2, *expert_down.shape[1:]),
        "sg": buf(*shared_gate.shape),
        "su": buf(*shared_up.shape),
        "sd": buf(*shared_down.shape),
        "gbuf": wide(line, sp_count, rows),
        "pair": wide(2 * rows, width),
        "kept": wide(2, *one),
        "core_out": buf(2, *one),
        "core_in": buf(2, *one),
        "x_out": buf(*one),
        "x_in": buf(*one),
        "base": wide(*one),
        "tok": buf(*per_level),
        "own": wide(*per_level),
        "ret_out": buf(*per_level),
        "up_in": buf(*per_level),
        "dn_in": buf(*per_level),
        "f_ref": wide(*forget_sums.shape[::-1]),
        "res_ref": buf(*one),
        "gain_ref": wide(1, width),
        "ids_ref": pltpu.VMEM(expert_ids.shape[::-1], jnp.int32),
        "score_ref": wide(*route_weights.shape[::-1]),
        "load_sem": dma(13),
        "weight_sem": dma(7),
        "side_send": dma(4),
        "q_recv": dma(1),
        "kv_send": dma(3),
        "kv_recv": dma(sp_count, 3),
        "back_send": dma(2),
        "back_recv": dma(2),
        "wy_send": dma(1),
        "wy_recv": dma(PIECES + EXTRA),
        "wx_send": dma(1),
        "wx_recv": dma(PIECES),
        "wc_sem": dma(2),
        "pair_sem": dma(2, 2),
        "hop_send": dma(1),
        "hop_recv": dma(ROW_PIECES),
        "tok_up": dma(1),
        "tok_dn": dma(1),
        "tok_recv": dma(line, ROW_PIECES),
        "gate_up": dma(1),
        "gate_dn": dma(1),
        "gate_recv": dma(line),
        "ret_send": dma(1),
        "up_recv": dma(line, ROW_PIECES),
        "dn_recv": dma(line, ROW_PIECES),
    }
    names = ins + ["out_ref"] + list(scratch)
    return pl.pallas_call(
        functools.partial(layer_kernel, names, sp_count, HEAD_DIM ** (-0.5)),
        out_shape=pltpu.VMEM(one, bf16),
        in_specs=[hbm] * 15,
        out_specs=pl.BlockSpec(memory_space=pltpu.VMEM),
        scratch_shapes=list(scratch.values()),
        compiler_params=pltpu.CompilerParams(
            collective_id=0, has_side_effects=True, vmem_limit_bytes=60 * 2**20
        ),
    )(
        queries,
        forget_sums.T,
        key_rows,
        value_rows,
        residual,
        norm_gain[None, :],
        expert_ids.T,
        route_weights.T,
        *loaded,
    )


def absorb_group(carried, query_group, shard_piece, sum_piece, score_scale):
    query_heads, query_sums, query_pos, last_pos = query_group
    key_piece, value_piece = shard_piece
    piece_rows = key_piece.shape[0]
    query_count, local_kv, group_size, head_size = query_heads.shape
    key_block = math.gcd(piece_rows, 1024)
    key_heads = key_piece.reshape(piece_rows, local_kv, head_size)
    value_heads = value_piece.reshape(piece_rows, local_kv, head_size)
    key_sums = sum_piece.reshape(piece_rows, local_kv, group_size).transpose(1, 2, 0)

    def update(block_start, held):
        row_max, row_sum, weighted = held
        key_part = lax.dynamic_slice_in_dim(key_heads, block_start, key_block, 0)
        value_part = lax.dynamic_slice_in_dim(value_heads, block_start, key_block, 0)
        sums_part = lax.dynamic_slice_in_dim(key_sums, block_start, key_block, 2)
        scores = (
            jnp.einsum("qhgd,khd->hgqk", query_heads, key_part, preferred_element_type=jnp.float32)
            * score_scale
        )
        scores = scores + (query_sums[:, :, :, None] - sums_part[:, :, None, :])
        key_pos = block_start + jnp.arange(key_block, dtype=jnp.int32)
        allowed = query_pos[:, None] >= key_pos[None, :]
        scores = jnp.where(allowed, scores, -jnp.inf)
        new_max = jnp.maximum(row_max, jnp.max(scores, axis=3))
        weights = jnp.exp(scores - new_max[:, :, :, None])
        factor = jnp.exp(row_max - new_max)
        row_sum = row_sum * factor + jnp.sum(weights, axis=3)
        products = jnp.einsum(
            "hgqk,khd->qhgd",
            weights.astype(jnp.bfloat16),
            value_part,
            preferred_element_type=jnp.float32,
        )
        weighted = weighted * factor.transpose(2, 0, 1)[:, :, :, None] + products
        return (new_max, row_sum, weighted)

    def one_block(block_index, held):
        block_start = block_index * key_block
        needed = block_start <= last_pos
        return lax.cond(needed, lambda inner: update(block_start, inner), lambda inner: inner, held)

    return lax.fori_loop(0, piece_rows // key_block, one_block, carried)


def finish(carried):
    row_max, row_sum, weighted = carried
    mixed = weighted / row_sum.transpose(2, 0, 1)[:, :, :, None]
    return mixed.reshape(mixed.shape[0], -1).astype(jnp.bfloat16)


def local(
    residual,
    queries,
    key_rows,
    value_rows,
    forget_sums,
    out_weight,
    norm_gain,
    expert_ids,
    route_weights,
    expert_gate,
    expert_up,
    expert_down,
    shared_gate,
    shared_up,
    shared_down,
):
    sp_count = lax.axis_size("sp")
    sp_index = lax.axis_index("sp")
    local_rows = queries.shape[0]
    local_kv = key_rows.shape[1] // HEAD_DIM
    group_size = HEADS // KV_HEADS
    score_scale = HEAD_DIM ** (-0.5)
    tp_count = lax.axis_size("tp")
    tokens_here = residual.shape[0]
    every_slot = 2 * tokens_here * TOPK >= tokens_here * expert_gate.shape[0] * sp_count
    if every_slot and expert_gate.shape[0] == 1 and sp_count == 8 and tp_count == 4:
        return layer_fused(
            residual,
            queries,
            key_rows,
            value_rows,
            forget_sums,
            norm_gain,
            expert_ids,
            route_weights,
            out_weight,
            expert_gate,
            expert_up,
            expert_down,
            shared_gate,
            shared_up,
            shared_down,
            sp_count,
        )
    own_first = sp_index * local_rows
    all_sums = lax.all_gather(forget_sums, "sp", axis=0, tiled=True)
    positions = own_first + jnp.arange(local_rows, dtype=jnp.int32)
    groups = [
        (
            queries.reshape(queries.shape[0], local_kv, group_size, HEAD_DIM),
            forget_sums.reshape(forget_sums.shape[0], local_kv, group_size).transpose(1, 2, 0),
            positions,
            positions[-1],
        )
    ]

    def initial(query_count):
        return (
            jnp.full((local_kv, group_size, query_count), -1e30, jnp.float32),
            jnp.zeros((local_kv, group_size, query_count), jnp.float32),
            jnp.zeros((query_count, local_kv, group_size, HEAD_DIM), jnp.float32),
        )

    def absorb(states, shard_piece):
        return tuple(
            (
                absorb_group(held, query_group, shard_piece, all_sums, score_scale)
                for held, query_group in zip(states, groups)
            )
        )

    start_states = tuple((initial(query_group[0].shape[0]) for query_group in groups))
    states = absorb(
        start_states,
        (
            lax.all_gather(key_rows, "sp", axis=0, tiled=True),
            lax.all_gather(value_rows, "sp", axis=0, tiled=True),
        ),
    )
    outputs = [finish(held) for held in states]
    attended = outputs[0]
    rows_out = local_rows // lax.axis_size("tp")
    branch = lax.psum_scatter(
        jnp.dot(attended, out_weight, preferred_element_type=jnp.float32).astype(jnp.bfloat16),
        "tp",
        scatter_dimension=0,
        tiled=True,
    ).astype(jnp.float32)
    stream = (residual.astype(jnp.float32) + branch).astype(jnp.bfloat16)
    wide = lax.optimization_barrier(stream).astype(jnp.float32)
    normed = (
        wide * lax.rsqrt(jnp.mean(wide * wide, axis=1, keepdims=True) + norm_eps) * norm_gain
    ).astype(jnp.bfloat16)
    width = normed.shape[1]
    experts_here = expert_gate.shape[0]
    total_experts = experts_here * sp_count
    capacity = 2 * rows_out * TOPK // total_experts
    flat_ids = expert_ids.reshape(-1)
    assigned = flat_ids.shape[0]
    onehot = (flat_ids[:, None] == jnp.arange(total_experts, dtype=jnp.int32)[None, :]).astype(
        jnp.int32
    )
    slot_rank = jnp.sum((jnp.cumsum(onehot, axis=0) - 1) * onehot, axis=1)
    target = flat_ids * capacity + slot_rank
    slot_count = total_experts * capacity
    source = (
        jnp.full((slot_count,), assigned, jnp.int32)
        .at[target]
        .set(jnp.arange(assigned, dtype=jnp.int32))
    )
    padded = jnp.concatenate([normed, jnp.zeros((1, width), jnp.bfloat16)], axis=0)
    outgoing = padded[source // TOPK].reshape(sp_count, experts_here, capacity, width)
    arrived = lax.all_to_all(outgoing, "sp", split_axis=0, concat_axis=0, tiled=True)
    gate_part = jnp.einsum(
        "necd,edf->necf", arrived, expert_gate, preferred_element_type=jnp.float32
    )
    up_part = jnp.einsum("necd,edf->necf", arrived, expert_up, preferred_element_type=jnp.float32)
    hidden = (jax.nn.silu(gate_part) * up_part).astype(jnp.bfloat16)
    processed = jnp.einsum(
        "necf,efd->necd", hidden, expert_down, preferred_element_type=jnp.float32
    ).astype(jnp.bfloat16)
    returned = lax.all_to_all(processed, "sp", split_axis=0, concat_axis=0, tiled=True)
    results = returned.reshape(slot_count, width)
    picked = results[target].reshape(rows_out, TOPK, width).astype(jnp.float32)
    gates = route_weights / jnp.sum(route_weights, axis=1, keepdims=True) * routed_scale
    routed = jnp.sum(gates[:, :, None] * picked, axis=1)
    shared_hidden = (
        jax.nn.silu(jnp.dot(normed, shared_gate, preferred_element_type=jnp.float32))
        * jnp.dot(normed, shared_up, preferred_element_type=jnp.float32)
    ).astype(jnp.bfloat16)
    shared_out = jnp.dot(shared_hidden, shared_down, preferred_element_type=jnp.float32)
    return (wide + shared_out + routed).astype(jnp.bfloat16)


def solution(mesh):
    in_specs = (
        P(("sp", "tp"), None),
        P("sp", "tp"),
        P("sp", "tp"),
        P("sp", "tp"),
        P("sp", "tp"),
        P("tp", None),
        P(),
        P(("sp", "tp"), None),
        P(("sp", "tp"), None),
        P("sp", None, None),
        P("sp", None, None),
        P("sp", None, None),
        P(),
        P(),
        P(),
    )
    out_specs = P(("sp", "tp"), None)
    return jax.shard_map(local, mesh=mesh, in_specs=in_specs, out_specs=out_specs, check_vma=False)
```

```python
import functools
import math
import types

import jax
import jax.numpy as jnp
from jax import lax
from jax.experimental import pallas as pl
from jax.experimental.pallas import tpu as pltpu
from jax.sharding import PartitionSpec as P

HEADS = 16
KV_HEADS = 8
HEAD_DIM = 128
TOPK = 4


routed_scale = 2.5
norm_eps = 1e-06


MESH_ID = pl.DeviceIdType.MESH
LOG2E = math.log2(math.e)


def remote(src, dst, send_sem, recv_sem, target):
    return pltpu.make_async_remote_copy(
        src_ref=src,
        dst_ref=dst,
        send_sem=send_sem,
        recv_sem=recv_sem,
        device_id=target,
        device_id_type=MESH_ID,
    )


def greet(barrier, target):
    pl.semaphore_signal(barrier, inc=1, device_id=target, device_id_type=MESH_ID)


PIECES = 8
EXTRA = 1
ROW_PIECES = 4


def aligned(start, size):
    return pl.ds(pl.multiple_of(start, size), size)


def layer_kernel(names, sp_count, score_scale, *refs):
    r = types.SimpleNamespace(**dict(zip(names, refs)))
    me, tp = lax.axis_index("sp"), lax.axis_index("tp")
    line = sp_count // 2
    last = line - 1
    z, y = me // 2, me % 2
    x, c = tp // 2, tp % 2
    mate_block = 2 * z + 1 - y
    mate = (mate_block, tp)
    above = (jnp.minimum(me + 2, sp_count - 1), tp)
    below = (jnp.maximum(me - 2, 0), tp)
    core_mate = (me, 2 * x + 1 - c)
    x_mate = (me, 2 * (1 - x) + c)
    not_last, not_first = z < last, z > 0
    q_rows = r.q_hbm.shape[0]
    rows, width = r.res_hbm.shape
    f32, bf16 = jnp.float32, jnp.bfloat16

    barrier = pltpu.get_barrier_semaphore()
    for peer in (mate, core_mate, x_mate):
        greet(barrier, peer)

    @pl.when(not_last)
    def _():
        greet(barrier, above)

    @pl.when(not_first)
    def _():
        greet(barrier, below)

    def lanes(ref, head):
        return ref.at[:, aligned(head * HEAD_DIM, HEAD_DIM)]

    def q_part(ref, j):
        return ref.at[pl.ds(j * q_rows, q_rows), :]

    loads = [
        (lanes(r.k_hbm, 1 - y), r.ksend),
        (lanes(r.v_hbm, 1 - y), r.vsend),
        (lanes(r.k_hbm, y), r.kbuf.at[me]),
        (lanes(r.v_hbm, y), r.vbuf.at[me]),
        (lanes(r.q_hbm, 2 * (1 - y)), q_part(r.qsend, 0)),
        (lanes(r.q_hbm, 2 * (1 - y) + 1), q_part(r.qsend, 1)),
        (lanes(r.q_hbm, 2 * y), q_part(r.qs.at[y], 0)),
        (lanes(r.q_hbm, 2 * y + 1), q_part(r.qs.at[y], 1)),
        (r.f_hbm, r.f_ref),
        (r.ids_hbm, r.ids_ref),
        (r.score_hbm, r.score_ref),
        (r.res_hbm, r.res_ref),
        (r.gain_hbm, r.gain_ref),
    ]
    loads = [pltpu.make_async_copy(a, b, r.load_sem.at[i]) for i, (a, b) in enumerate(loads)]
    for copy in loads:
        copy.start()
    sources = (r.wo_hbm, r.eg_hbm, r.eu_hbm, r.ed_hbm, r.sg_hbm, r.su_hbm, r.sd_hbm)
    held = (r.wo, r.eg.at[0], r.eu.at[0], r.ed.at[0], r.sg, r.su, r.sd)
    weights = [pltpu.make_async_copy(a, b, r.weight_sem.at[i]) for i, (a, b) in enumerate(zip(sources, held))]
    r.acc[...] = jnp.zeros(r.acc.shape, f32)
    r.den[...] = jnp.zeros(r.den.shape, f32)
    r.top[...] = jnp.full(r.top.shape, -jnp.inf, f32)
    r.fsend[...] = jnp.zeros(r.fsend.shape, f32)
    r.fbuf[me] = jnp.zeros(r.fsend.shape, f32)
    for copy in [loads[8]] + loads[:8]:
        copy.wait()
    first_f, second_f = r.f_ref[0:2, :], r.f_ref[2:4, :]
    r.fsend[0:2, :] = jnp.where(y == 0, second_f, first_f)
    r.fbuf[me, 0:2, :] = jnp.where(y == 0, first_f, second_f)
    pl.semaphore_wait(barrier, 3 + not_last.astype(jnp.int32) + not_first.astype(jnp.int32))

    def side_moves(block, sources):
        bufs = (r.fbuf, r.kbuf, r.vbuf)
        return [
            remote(a, b.at[block], r.side_send.at[i], r.kv_recv.at[block, i], mate)
            for i, (a, b) in enumerate(zip(sources, bufs))
        ]

    def up_moves(block, target):
        return [
            remote(b.at[block], b.at[block], r.kv_send.at[i], r.kv_recv.at[block, i], target)
            for i, b in enumerate((r.fbuf, r.kbuf, r.vbuf))
        ]

    def pass_up(block):
        @pl.when(not_last)
        def _():
            for copy in up_moves(block, above):
                copy.start()

    def q_move(slot):
        return remote(r.qsend, r.qs.at[slot], r.side_send.at[3], r.q_recv.at[0], mate)

    def parts(refs, quarter, i):
        g, u, d = refs
        tall, flat, wide = g.shape[0] // 4 // PIECES, d.shape[0] // 4, d.shape[1] // PIECES
        span = aligned((quarter * PIECES + i) * tall, tall)
        return (g.at[span, :], u.at[span, :], d.at[aligned(quarter * flat, flat), aligned(i * wide, wide)])

    own_expert = (r.eg.at[0], r.eu.at[0], r.ed.at[0])
    mates_expert = (r.eg.at[1], r.eu.at[1], r.ed.at[1])

    def w_moves(sources, quarter, i, send, recv, target):
        return [
            remote(a, b, send, recv, target)
            for a, b in zip(parts(sources, quarter, i), parts(mates_expert, quarter, i))
        ]

    third = r.eg.shape[1] // 4 // PIECES
    last_hop = PIECES - EXTRA - 1

    def w_all(thirds, send, recv, target):
        one = r.eg.at[1, 0 : thirds * third, :]
        return remote(one, one, send, recv, target)

    def w_core_all():
        both = r.eg.at[:, 0 : PIECES * 3 * third, :]
        return remote(both, both, r.wc_sem.at[0], r.wc_sem.at[1], core_mate)

    x_quarter = 2 * (1 - x) + c

    def issue_weights(start, stop):
        def one(i, _):
            for copy in w_moves(own_expert, tp, i, r.wy_send.at[0], r.wy_recv.at[i], mate):
                copy.start()
            return 0

        lax.fori_loop(start, stop, one, 0)

    def issue_extra():
        by_y = w_moves(own_expert, x_quarter, last_hop, r.wy_send.at[0], r.wy_recv.at[PIECES], mate)[2:]
        for i in range(PIECES - EXTRA, PIECES):
            by_y += w_moves(own_expert, x_quarter, i, r.wy_send.at[0], r.wy_recv.at[EXTRA + i + 1], mate)
        for copy in by_y:
            copy.start()

    def to_core(i, quarter):
        for copy in w_moves(mates_expert, quarter, i, r.wc_sem.at[0], r.wc_sem.at[1], core_mate):
            copy.start()

    def spread(start, stop):
        def one(i, _):
            w_all(3, r.wy_send.at[0], r.wy_recv.at[i], mate).wait_recv()

            hops = w_moves(mates_expert, tp, i, r.wx_send.at[0], r.wx_recv.at[i], x_mate)

            @pl.when(i <= last_hop)
            def _():
                for copy in hops[:2]:
                    copy.start()

            @pl.when(i < last_hop)
            def _():
                hops[2].start()

            to_core(i, tp)
            return 0

        lax.fori_loop(start, stop, one, 0)

    def spread_x(start, stop):
        def one(i, _):
            w_all(3, r.wx_send.at[0], r.wx_recv.at[i], x_mate).wait_recv()
            to_core(i, x_quarter)
            return 0

        lax.fori_loop(start, stop, one, 0)

    def at_z(*values):
        out = values[-1]
        for level in range(len(values) - 1):
            out = jnp.where(z == level, values[level], out)
        return out

    early = at_z(2, 2, 3, 5)
    for copy in side_moves(me, (r.fsend, r.ksend, r.vsend)):
        copy.start()
    pass_up(me)
    for copy in weights[1:4]:
        copy.start()
    for copy in loads[9:]:
        copy.wait()
    scores = r.score_ref[...]
    gates = scores / jnp.sum(scores, axis=0, keepdims=True) * routed_scale
    for e in range(sp_count):
        r.gbuf[z, e : e + 1, :] = jnp.sum(jnp.where(r.ids_ref[...] == e, gates, 0.0), axis=0, keepdims=True)

    def absorb(i, block, masked):
        q_block = 2 * z + i
        keys, values = r.kbuf[block], r.vbuf[block]
        for j in range(2):
            span = slice(j * q_rows, (j + 1) * q_rows)
            products = lax.dot_general(
                keys, r.qs[i, span, :], (((1,), (1,)), ((), ())), preferred_element_type=f32
            )
            column = jnp.broadcast_to(r.fbuf[block, j : j + 1, :], (HEAD_DIM, q_rows)).T
            column = jnp.concatenate([column] * (q_rows // HEAD_DIM), axis=1)
            drop = r.fbuf[q_block, j : j + 1, :] - column
            part = products * (score_scale * LOG2E) + drop * LOG2E
            if masked:
                at_key = lax.broadcasted_iota(jnp.int32, part.shape, 0)
                at_query = lax.broadcasted_iota(jnp.int32, part.shape, 1)
                part = jnp.where(at_query >= at_key, part, -jnp.inf)
            old = r.top[i, :1, span]
            peak = jnp.maximum(old, jnp.max(part, axis=0, keepdims=True))
            factor = jnp.exp2(old - peak)
            w = jnp.exp2(part - peak)
            r.den[i, :1, span] = r.den[i, :1, span] * factor + jnp.sum(w, axis=0, keepdims=True)
            mixed = lax.dot_general(
                values, w.astype(bf16), (((0,), (0,)), ((), ())), preferred_element_type=f32
            )
            r.acc[i, :, span] = r.acc[i, :, span] * factor + mixed
            r.top[i, :1, span] = peak

    absorb(y, me, True)
    q_move(y).start()
    for copy in weights[1:4]:
        copy.wait()
    issue_weights(0, early)
    for copy in weights[:1] + weights[4:]:
        copy.start()
    def pick(turn, values):
        out = values[-1]
        for k in range(len(values) - 1):
            out = jnp.where(turn == k, values[k], out)
        return out

    def turn_block(turn):
        level = at_z(0, 0, pick(turn, (1, 0, 1, 0)), pick(turn, (2, 1, 2, 0, 1, 0)))
        other = at_z(0, pick(turn, (0, 1)), pick(turn, (0, 0, 1, 1)), pick(turn, (0, 0, 1, 0, 1, 1)))
        return 2 * level + jnp.where(other == 0, y, 1 - y)

    def take_keys(turn):
        block = turn_block(turn)
        for copy in up_moves(block, below):
            copy.wait_recv()
        pass_up(block)

    @pl.when(not_first)
    def _():
        take_keys(0)

    for copy in side_moves(mate_block, (r.fsend, r.ksend, r.vsend)):
        copy.wait_recv()
    pass_up(mate_block)

    @pl.when(not_first)
    def _():
        take_keys(1)

    q_move(1 - y).wait_recv()
    absorb(1 - y, mate_block, True)
    absorb(1, 2 * z, False)

    def take(turn, _):
        ahead = jnp.where(z == last, turn, turn + 1)

        @pl.when(jnp.logical_and(ahead >= 2, ahead < 2 * z))
        def _():
            take_keys(ahead)

        block = turn_block(turn)
        absorb(1 - y, block, False)

        @pl.when(turn < 2 * z - 1)
        def _():
            absorb(y, block, False)

        @pl.when(turn == 0)
        def _():
            spread(0, 1)

        @pl.when(jnp.logical_and(z >= last - 1, turn == 2))
        def _():
            spread(1, 2)

        @pl.when(jnp.logical_and(z == last, turn == 3))
        def _():
            spread(2, 3)

        return 0

    lax.fori_loop(0, 2 * z, take, 0)

    def finish(i, target):
        for j in range(2):
            span = slice(j * q_rows, (j + 1) * q_rows)
            done = (r.acc[i, :, span] / r.den[i, :1, span]).T
            target[:, j * HEAD_DIM : (j + 1) * HEAD_DIM] = done.astype(bf16)

    far, near = (1 - x) * 2, x * 2

    def back_move(slot, i):
        span = aligned((far if i == 0 else near) * rows, 2 * rows)
        return remote(r.attsend.at[span, :], r.att.at[slot, span, :], r.back_send.at[i], r.back_recv.at[i], mate)

    finish(1 - y, r.attsend)
    for i in range(2):
        back_move(y, i).start()
    issue_weights(early, PIECES)
    issue_extra()

    @pl.when(not_first)
    def _():
        absorb(y, 1 - y, False)

    finish(y, r.att.at[y])
    marks = [at_z(0, 1, 2, 3), at_z(2, 2, 3, 5), at_z(3, 3, 4, 6), at_z(6, 4, 6, 7), at_z(8, 6, 7, 8), at_z(8, 7, 8, 8)]
    x_mark = at_z(1, 2, 3, 4)
    spread(marks[0], marks[1])

    weights[0].wait()
    half = r.att.shape[2]

    def core_copy(i):
        return remote(r.core_out.at[i], r.core_in.at[i], r.pair_sem.at[0, i], r.pair_sem.at[1, i], core_mate)

    part_rows = rows // ROW_PIECES

    def piece(ref, p):
        return ref.at[pl.ds(p * part_rows, part_rows), :]

    def hop(p):
        return remote(piece(r.x_out, p), piece(r.x_in, p), r.hop_send.at[0], r.hop_recv.at[p], x_mate)

    def project_to(i, _):
        out_x = jnp.where(i == 0, far, near)
        back = remote(
            r.attsend.at[0 : 2 * rows, :], r.attsend.at[0 : 2 * rows, :], r.back_send.at[i], r.back_recv.at[i], mate
        )
        back.wait_recv()
        span = aligned(out_x * rows, 2 * rows)
        r.pair[...] = jnp.dot(
            r.att[0, span, :], r.wo[0:half, :], preferred_element_type=f32
        ) + jnp.dot(r.att[1, span, :], r.wo[half : 2 * half, :], preferred_element_type=f32)
        r.core_out[i] = r.pair[aligned((1 - c) * rows, rows), :].astype(bf16)
        core_copy(i).start()
        r.kept[i] = r.pair[aligned(c * rows, rows), :]
        return 0

    lax.fori_loop(0, 2, project_to, 0)
    core_copy(0).wait_recv()
    for p in range(ROW_PIECES):
        span = slice(p * part_rows, (p + 1) * part_rows)
        r.x_out[span, :] = (r.kept[0, span, :] + r.core_in[0, span, :].astype(f32)).astype(bf16)
        hop(p).start()
    core_copy(1).wait_recv()
    spread(marks[1], marks[2])

    def tok_move(level, p, send, target):
        return remote(
            piece(r.tok.at[level], p), piece(r.tok.at[level], p), send.at[0], r.tok_recv.at[level, p], target
        )

    def gate_move(level, send, target):
        return remote(r.gbuf.at[level], r.gbuf.at[level], send.at[0], r.gate_recv.at[level], target)

    def arrive_piece(level, p):
        @pl.when(level < z)
        def _():
            if p == 0:
                gate_move(level, r.gate_up, below).wait_recv()
            tok_move(level, p, r.tok_up, below).wait_recv()

            @pl.when(not_last)
            def _():
                if p == 0:
                    gate_move(level, r.gate_up, above).start()
                tok_move(level, p, r.tok_up, above).start()

        @pl.when(level > z)
        def _():
            if p == 0:
                gate_move(level, r.gate_dn, above).wait_recv()
            tok_move(level, p, r.tok_dn, above).wait_recv()

            @pl.when(not_first)
            def _():
                if p == 0:
                    gate_move(level, r.gate_dn, below).start()
                tok_move(level, p, r.tok_dn, below).start()

    def arrive(level):
        for p in range(ROW_PIECES):
            arrive_piece(level, p)

    @pl.when(not_last)
    def _():
        gate_move(z, r.gate_up, above).start()

    @pl.when(not_first)
    def _():
        gate_move(z, r.gate_dn, below).start()

    for p in range(ROW_PIECES):
        span = slice(p * part_rows, (p + 1) * part_rows)
        branch = r.kept[1, span, :] + r.core_in[1, span, :].astype(f32) + r.res_ref[span, :].astype(f32)
        hop(p).wait_recv()
        stream = (branch + r.x_in[span, :].astype(f32)).astype(bf16)
        wide = stream.astype(f32)
        scale = lax.rsqrt(jnp.mean(wide * wide, axis=1, keepdims=True) + norm_eps)
        r.tok[z, span, :] = (wide * scale * r.gain_ref[...]).astype(bf16)
        r.base[span, :] = wide

        @pl.when(not_last)
        def _():
            tok_move(z, p, r.tok_up, above).start()

        @pl.when(not_first)
        def _():
            tok_move(z, p, r.tok_dn, below).start()

    spread(marks[2], marks[3])
    spread_x(0, x_mark)
    for copy in weights[4:]:
        copy.wait()

    def gated(inputs, gate, up, down):
        first = jnp.dot(inputs, gate[...], preferred_element_type=f32)
        second = jnp.dot(inputs, up[...], preferred_element_type=f32)
        hidden = (first / (1.0 + jnp.exp(-first)) * second).astype(bf16)
        return jnp.dot(hidden, down[...], preferred_element_type=f32)

    def expert(level, slot, number, start, count):
        table = r.gbuf[level]
        at_expert = lax.broadcasted_iota(jnp.int32, table.shape, 0) == number
        row = jnp.sum(jnp.where(at_expert, table, 0.0), axis=0, keepdims=True)
        shape = (count, row.shape[1])
        diagonal = lax.broadcasted_iota(jnp.int32, shape, 0) + start == lax.broadcasted_iota(jnp.int32, shape, 1)
        column = jnp.sum(jnp.where(diagonal, row, 0.0), axis=1, keepdims=True)
        inputs = r.tok[level, pl.ds(start, count), :]
        result = gated(inputs, r.eg.at[slot], r.eu.at[slot], r.ed.at[slot])
        return result.astype(bf16).astype(f32) * column

    def up_back(level, p):
        return remote(
            piece(r.ret_out.at[level], p), piece(r.up_in.at[level], p), r.ret_send.at[0], r.up_recv.at[level, p], above
        )

    def dn_back(level, p):
        return remote(
            piece(r.ret_out.at[level], p), piece(r.dn_in.at[level], p), r.ret_send.at[0], r.dn_recv.at[level, p], below
        )

    def give_piece(level, p):
        span = pl.ds(p * part_rows, part_rows)

        def send(back, came, chained):
            @pl.when(chained)
            def _():
                back(level, p).wait_recv()
                r.ret_out[level, span, :] = (r.own[level, span, :] + came[level, span, :].astype(f32)).astype(bf16)

            @pl.when(jnp.logical_not(chained))
            def _():
                r.ret_out[level, span, :] = r.own[level, span, :].astype(bf16)

            back(level, p).start()

        @pl.when(level > z)
        def _():
            send(up_back, r.up_in, not_first)

        @pl.when(level < z)
        def _():
            send(dn_back, r.dn_in, not_last)

    def give_back(level):
        for p in range(ROW_PIECES):
            give_piece(level, p)

    def own_expert_on(level):
        r.own[level] = expert(level, 0, me, 0, rows)

    def mates_expert_on(level):
        r.own[level] += expert(level, 1, mate_block, 0, rows)

    def first_turns(k, _):
        level = jnp.where(k == 0, at_z(1, 0, 0, 2), at_z(2, 2, 1, 0))

        for p in range(ROW_PIECES):
            arrive_piece(level, p)

            @pl.when(jnp.logical_and(z == last - 1, k == 1))
            def _():
                arrive_piece(last, p)

        spread(jnp.where(k == 0, marks[3], marks[4]), jnp.where(k == 0, marks[4], marks[5]))
        own_expert_on(level)
        return 0

    at_end = jnp.logical_or(z == 0, z == last)

    def self_turn():
        own_expert_on(z)
        r.base[...] += gated(r.tok[z], r.sg, r.su, r.sd)

    @pl.when(at_end)
    def _():
        self_turn()

    lax.fori_loop(0, 2, first_turns, 0)

    @pl.when(jnp.logical_not(at_end))
    def _():
        self_turn()

    spread(marks[5], PIECES)

    @pl.when(jnp.logical_and(not_first, not_last))
    def _():
        @pl.when(z == 1)
        def _():
            arrive(last)

        own_expert_on(last)

    spread_x(x_mark, last_hop)
    w_all(2, r.wx_send.at[0], r.wx_recv.at[last_hop], x_mate).wait_recv()
    w_all(1, r.wy_send.at[0], r.wy_recv.at[PIECES], mate).wait_recv()
    to_core(last_hop, x_quarter)
    for i in range(PIECES - EXTRA, PIECES):
        w_all(3, r.wy_send.at[0], r.wy_recv.at[EXTRA + i + 1], mate).wait_recv()
        to_core(i, x_quarter)
    w_core_all().wait_recv()

    def second_turns(k, _):
        level = at_z(pick(k, (2, 1, 3)), pick(k, (2, 0, 3)), pick(k, (0, 1, 3)), k)

        @pl.when(jnp.logical_and(z == last, k == 1))
        def _():
            arrive(level)
            own_expert_on(level)

        mates_expert_on(level)

        @pl.when(z == last)
        def _():
            give_back(level)

        @pl.when(jnp.logical_and(z == 0, k == 0))
        def _():
            for p in range(ROW_PIECES // 2):
                give_piece(level, p)

        return 0

    lax.fori_loop(0, jnp.where(z == 0, line - 2, line - 1), second_turns, 0)

    @pl.when(z == 0)
    def _():
        def one_half(i, _):
            start, count = i * (rows // 2), rows // 2
            for p in range(ROW_PIECES):

                @pl.when(p // (ROW_PIECES // 2) == i)
                def _():
                    arrive_piece(last, p)

            both = expert(last, 0, me, start, count) + expert(last, 1, mate_block, start, count)
            r.own[last, pl.ds(start, count), :] = both
            for p in range(ROW_PIECES):

                @pl.when(p // (ROW_PIECES // 2) == i)
                def _():
                    give_piece(last, p)

            return 0

        lax.fori_loop(0, 2, one_half, 0)
        for p in range(ROW_PIECES // 2, ROW_PIECES):
            give_piece(last - 1, p)


    @pl.when(z != 1)
    def _():
        give_back(at_z(1, 1, 0, z))

    @pl.when(z == 1)
    def _():
        for p in range(ROW_PIECES // 2):
            give_piece(2, p)

    mates_expert_on(z)
    r.base[...] += r.own[z]

    @pl.when(jnp.logical_and(not_first, not_last))
    def _():
        lag = 2
        for step in range(ROW_PIECES + lag):

            @pl.when(z == 1)
            def _():
                if step < ROW_PIECES:
                    give_piece(0, step)
                    give_piece(last, step)
                else:
                    give_piece(2, step - ROW_PIECES // 2)

            @pl.when(z == last - 1)
            def _():
                if step < ROW_PIECES:
                    give_piece(1, step)
                if step >= lag:
                    give_piece(last, step - lag)

    for p in range(ROW_PIECES):
        span = slice(p * part_rows, (p + 1) * part_rows)

        @pl.when(not_first)
        def _():
            up_back(z, p).wait_recv()
            r.base[span, :] += r.up_in[z, span, :].astype(f32)

        @pl.when(not_last)
        def _():
            dn_back(z, p).wait_recv()
            r.base[span, :] += r.dn_in[z, span, :].astype(f32)

        r.out_ref[span, :] = r.base[span, :].astype(bf16)

    for copy in side_moves(me, (r.fsend, r.ksend, r.vsend)) + [q_move(y), back_move(y, 0), back_move(y, 1)]:
        copy.wait_send()
    for i in range(2):
        core_copy(i).wait_send()
    def sent(whole, send, recv, target):
        remote(whole, whole, send, recv, target).wait_send()

    sent(r.x_out, r.hop_send.at[0], r.hop_recv.at[0], x_mate)
    w_all(3 * (PIECES + EXTRA) + 1, r.wy_send.at[0], r.wy_recv.at[0], mate).wait_send()
    w_all(3 * (PIECES - EXTRA) - 1, r.wx_send.at[0], r.wx_recv.at[0], x_mate).wait_send()
    w_core_all().wait_send()
    done = pl.ds(0, line - 1)

    @pl.when(not_last)
    def _():
        for level in range(last):

            @pl.when(z == level)
            def _():
                blocks, levels = pl.ds(0, 2 * level + 2), pl.ds(0, level + 1)
                for i, b in enumerate((r.fbuf, r.kbuf, r.vbuf)):
                    sent(b.at[blocks], r.kv_send.at[i], r.kv_recv.at[0, i], above)
                sent(r.gbuf.at[levels], r.gate_up.at[0], r.gate_recv.at[0], above)
                sent(r.tok.at[levels], r.tok_up.at[0], r.tok_recv.at[0, 0], above)

    @pl.when(not_first)
    def _():
        for level in range(1, line):

            @pl.when(z == level)
            def _():
                levels = pl.ds(0, line - level)
                sent(r.gbuf.at[levels], r.gate_dn.at[0], r.gate_recv.at[0], below)
                sent(r.tok.at[levels], r.tok_dn.at[0], r.tok_recv.at[0, 0], below)

    sent(r.ret_out.at[done], r.ret_send.at[0], r.up_recv.at[0, 0], above)


def layer_fused(
    residual,
    queries,
    key_rows,
    value_rows,
    forget_sums,
    norm_gain,
    expert_ids,
    route_weights,
    out_weight,
    expert_gate,
    expert_up,
    expert_down,
    shared_gate,
    shared_up,
    shared_down,
    sp_count,
):
    q_rows, features = queries.shape
    rows, width = residual.shape
    line = sp_count // 2
    bf16, f32 = jnp.bfloat16, jnp.float32
    hbm = pl.BlockSpec(memory_space=pl.ANY)
    loaded = (
        out_weight,
        expert_gate[0],
        expert_up[0],
        expert_down[0],
        shared_gate,
        shared_up,
        shared_down,
    )
    ins = ["q_hbm", "f_hbm", "k_hbm", "v_hbm", "res_hbm", "gain_hbm", "ids_hbm", "score_hbm"]
    ins += ["wo_hbm", "eg_hbm", "eu_hbm", "ed_hbm", "sg_hbm", "su_hbm", "sd_hbm"]
    one, per_level = (rows, width), (line, rows, width)
    stacked = (2 * q_rows, HEAD_DIM)

    def buf(*shape):
        return pltpu.VMEM(shape, bf16)

    def wide(*shape):
        return pltpu.VMEM(shape, f32)

    def dma(*shape):
        return pltpu.SemaphoreType.DMA(shape)

    scratch = {
        "qs": buf(2, *stacked),
        "qsend": buf(*stacked),
        "kbuf": buf(sp_count, q_rows, HEAD_DIM),
        "vbuf": buf(sp_count, q_rows, HEAD_DIM),
        "fbuf": wide(sp_count, 8, q_rows),
        "ksend": buf(q_rows, HEAD_DIM),
        "vsend": buf(q_rows, HEAD_DIM),
        "fsend": wide(8, q_rows),
        "acc": wide(2, HEAD_DIM, 2 * q_rows),
        "top": wide(2, 8, 2 * q_rows),
        "den": wide(2, 8, 2 * q_rows),
        "att": buf(2, q_rows, features // 2),
        "attsend": buf(q_rows, features // 2),
        "wo": buf(*out_weight.shape),
        "eg": buf(2, *expert_gate.shape[1:]),
        "eu": buf(2, *expert_up.shape[1:]),
        "ed": buf(2, *expert_down.shape[1:]),
        "sg": buf(*shared_gate.shape),
        "su": buf(*shared_up.shape),
        "sd": buf(*shared_down.shape),
        "gbuf": wide(line, sp_count, rows),
        "pair": wide(2 * rows, width),
        "kept": wide(2, *one),
        "core_out": buf(2, *one),
        "core_in": buf(2, *one),
        "x_out": buf(*one),
        "x_in": buf(*one),
        "base": wide(*one),
        "tok": buf(*per_level),
        "own": wide(*per_level),
        "ret_out": buf(*per_level),
        "up_in": buf(*per_level),
        "dn_in": buf(*per_level),
        "f_ref": wide(*forget_sums.shape[::-1]),
        "res_ref": buf(*one),
        "gain_ref": wide(1, width),
        "ids_ref": pltpu.VMEM(expert_ids.shape[::-1], jnp.int32),
        "score_ref": wide(*route_weights.shape[::-1]),
        "load_sem": dma(13),
        "weight_sem": dma(7),
        "side_send": dma(4),
        "q_recv": dma(1),
        "kv_send": dma(3),
        "kv_recv": dma(sp_count, 3),
        "back_send": dma(2),
        "back_recv": dma(2),
        "wy_send": dma(1),
        "wy_recv": dma(PIECES + EXTRA + 1),
        "wx_send": dma(1),
        "wx_recv": dma(PIECES),
        "wc_sem": dma(2),
        "pair_sem": dma(2, 2),
        "hop_send": dma(1),
        "hop_recv": dma(ROW_PIECES),
        "tok_up": dma(1),
        "tok_dn": dma(1),
        "tok_recv": dma(line, ROW_PIECES),
        "gate_up": dma(1),
        "gate_dn": dma(1),
        "gate_recv": dma(line),
        "ret_send": dma(1),
        "up_recv": dma(line, ROW_PIECES),
        "dn_recv": dma(line, ROW_PIECES),
    }
    names = ins + ["out_ref"] + list(scratch)
    return pl.pallas_call(
        functools.partial(layer_kernel, names, sp_count, HEAD_DIM ** (-0.5)),
        out_shape=pltpu.VMEM(one, bf16),
        in_specs=[hbm] * 15,
        out_specs=pl.BlockSpec(memory_space=pltpu.VMEM),
        scratch_shapes=list(scratch.values()),
        compiler_params=pltpu.CompilerParams(
            collective_id=0, has_side_effects=True, vmem_limit_bytes=60 * 2**20
        ),
    )(
        queries,
        forget_sums.T,
        key_rows,
        value_rows,
        residual,
        norm_gain[None, :],
        expert_ids.T,
        route_weights.T,
        *loaded,
    )


def absorb_group(carried, query_group, shard_piece, sum_piece, score_scale):
    query_heads, query_sums, query_pos, last_pos = query_group
    key_piece, value_piece = shard_piece
    piece_rows = key_piece.shape[0]
    query_count, local_kv, group_size, head_size = query_heads.shape
    key_block = math.gcd(piece_rows, 1024)
    key_heads = key_piece.reshape(piece_rows, local_kv, head_size)
    value_heads = value_piece.reshape(piece_rows, local_kv, head_size)
    key_sums = sum_piece.reshape(piece_rows, local_kv, group_size).transpose(1, 2, 0)

    def update(block_start, held):
        row_max, row_sum, weighted = held
        key_part = lax.dynamic_slice_in_dim(key_heads, block_start, key_block, 0)
        value_part = lax.dynamic_slice_in_dim(value_heads, block_start, key_block, 0)
        sums_part = lax.dynamic_slice_in_dim(key_sums, block_start, key_block, 2)
        scores = (
            jnp.einsum("qhgd,khd->hgqk", query_heads, key_part, preferred_element_type=jnp.float32)
            * score_scale
        )
        scores = scores + (query_sums[:, :, :, None] - sums_part[:, :, None, :])
        key_pos = block_start + jnp.arange(key_block, dtype=jnp.int32)
        allowed = query_pos[:, None] >= key_pos[None, :]
        scores = jnp.where(allowed, scores, -jnp.inf)
        new_max = jnp.maximum(row_max, jnp.max(scores, axis=3))
        weights = jnp.exp(scores - new_max[:, :, :, None])
        factor = jnp.exp(row_max - new_max)
        row_sum = row_sum * factor + jnp.sum(weights, axis=3)
        products = jnp.einsum(
            "hgqk,khd->qhgd",
            weights.astype(jnp.bfloat16),
            value_part,
            preferred_element_type=jnp.float32,
        )
        weighted = weighted * factor.transpose(2, 0, 1)[:, :, :, None] + products
        return (new_max, row_sum, weighted)

    def one_block(block_index, held):
        block_start = block_index * key_block
        needed = block_start <= last_pos
        return lax.cond(needed, lambda inner: update(block_start, inner), lambda inner: inner, held)

    return lax.fori_loop(0, piece_rows // key_block, one_block, carried)


def finish(carried):
    row_max, row_sum, weighted = carried
    mixed = weighted / row_sum.transpose(2, 0, 1)[:, :, :, None]
    return mixed.reshape(mixed.shape[0], -1).astype(jnp.bfloat16)


def local(
    residual,
    queries,
    key_rows,
    value_rows,
    forget_sums,
    out_weight,
    norm_gain,
    expert_ids,
    route_weights,
    expert_gate,
    expert_up,
    expert_down,
    shared_gate,
    shared_up,
    shared_down,
):
    sp_count = lax.axis_size("sp")
    sp_index = lax.axis_index("sp")
    local_rows = queries.shape[0]
    local_kv = key_rows.shape[1] // HEAD_DIM
    group_size = HEADS // KV_HEADS
    score_scale = HEAD_DIM ** (-0.5)
    tp_count = lax.axis_size("tp")
    tokens_here = residual.shape[0]
    every_slot = 2 * tokens_here * TOPK >= tokens_here * expert_gate.shape[0] * sp_count
    if every_slot and expert_gate.shape[0] == 1 and sp_count == 8 and tp_count == 4:
        return layer_fused(
            residual,
            queries,
            key_rows,
            value_rows,
            forget_sums,
            norm_gain,
            expert_ids,
            route_weights,
            out_weight,
            expert_gate,
            expert_up,
            expert_down,
            shared_gate,
            shared_up,
            shared_down,
            sp_count,
        )
    own_first = sp_index * local_rows
    all_sums = lax.all_gather(forget_sums, "sp", axis=0, tiled=True)
    positions = own_first + jnp.arange(local_rows, dtype=jnp.int32)
    groups = [
        (
            queries.reshape(queries.shape[0], local_kv, group_size, HEAD_DIM),
            forget_sums.reshape(forget_sums.shape[0], local_kv, group_size).transpose(1, 2, 0),
            positions,
            positions[-1],
        )
    ]

    def initial(query_count):
        return (
            jnp.full((local_kv, group_size, query_count), -1e30, jnp.float32),
            jnp.zeros((local_kv, group_size, query_count), jnp.float32),
            jnp.zeros((query_count, local_kv, group_size, HEAD_DIM), jnp.float32),
        )

    def absorb(states, shard_piece):
        return tuple(
            (
                absorb_group(held, query_group, shard_piece, all_sums, score_scale)
                for held, query_group in zip(states, groups)
            )
        )

    start_states = tuple((initial(query_group[0].shape[0]) for query_group in groups))
    states = absorb(
        start_states,
        (
            lax.all_gather(key_rows, "sp", axis=0, tiled=True),
            lax.all_gather(value_rows, "sp", axis=0, tiled=True),
        ),
    )
    outputs = [finish(held) for held in states]
    attended = outputs[0]
    rows_out = local_rows // lax.axis_size("tp")
    branch = lax.psum_scatter(
        jnp.dot(attended, out_weight, preferred_element_type=jnp.float32).astype(jnp.bfloat16),
        "tp",
        scatter_dimension=0,
        tiled=True,
    ).astype(jnp.float32)
    stream = (residual.astype(jnp.float32) + branch).astype(jnp.bfloat16)
    wide = lax.optimization_barrier(stream).astype(jnp.float32)
    normed = (
        wide * lax.rsqrt(jnp.mean(wide * wide, axis=1, keepdims=True) + norm_eps) * norm_gain
    ).astype(jnp.bfloat16)
    width = normed.shape[1]
    experts_here = expert_gate.shape[0]
    total_experts = experts_here * sp_count
    capacity = 2 * rows_out * TOPK // total_experts
    flat_ids = expert_ids.reshape(-1)
    assigned = flat_ids.shape[0]
    onehot = (flat_ids[:, None] == jnp.arange(total_experts, dtype=jnp.int32)[None, :]).astype(
        jnp.int32
    )
    slot_rank = jnp.sum((jnp.cumsum(onehot, axis=0) - 1) * onehot, axis=1)
    target = flat_ids * capacity + slot_rank
    slot_count = total_experts * capacity
    source = (
        jnp.full((slot_count,), assigned, jnp.int32)
        .at[target]
        .set(jnp.arange(assigned, dtype=jnp.int32))
    )
    padded = jnp.concatenate([normed, jnp.zeros((1, width), jnp.bfloat16)], axis=0)
    outgoing = padded[source // TOPK].reshape(sp_count, experts_here, capacity, width)
    arrived = lax.all_to_all(outgoing, "sp", split_axis=0, concat_axis=0, tiled=True)
    gate_part = jnp.einsum(
        "necd,edf->necf", arrived, expert_gate, preferred_element_type=jnp.float32
    )
    up_part = jnp.einsum("necd,edf->necf", arrived, expert_up, preferred_element_type=jnp.float32)
    hidden = (jax.nn.silu(gate_part) * up_part).astype(jnp.bfloat16)
    processed = jnp.einsum(
        "necf,efd->necd", hidden, expert_down, preferred_element_type=jnp.float32
    ).astype(jnp.bfloat16)
    returned = lax.all_to_all(processed, "sp", split_axis=0, concat_axis=0, tiled=True)
    results = returned.reshape(slot_count, width)
    picked = results[target].reshape(rows_out, TOPK, width).astype(jnp.float32)
    gates = route_weights / jnp.sum(route_weights, axis=1, keepdims=True) * routed_scale
    routed = jnp.sum(gates[:, :, None] * picked, axis=1)
    shared_hidden = (
        jax.nn.silu(jnp.dot(normed, shared_gate, preferred_element_type=jnp.float32))
        * jnp.dot(normed, shared_up, preferred_element_type=jnp.float32)
    ).astype(jnp.bfloat16)
    shared_out = jnp.dot(shared_hidden, shared_down, preferred_element_type=jnp.float32)
    return (wide + shared_out + routed).astype(jnp.bfloat16)


def solution(mesh):
    in_specs = (
        P(("sp", "tp"), None),
        P("sp", "tp"),
        P("sp", "tp"),
        P("sp", "tp"),
        P("sp", "tp"),
        P("tp", None),
        P(),
        P(("sp", "tp"), None),
        P(("sp", "tp"), None),
        P("sp", None, None),
        P("sp", None, None),
        P("sp", None, None),
        P(),
        P(),
        P(),
    )
    out_specs = P(("sp", "tp"), None)
    return jax.shard_map(local, mesh=mesh, in_specs=in_specs, out_specs=out_specs, check_vma=False)
```
